32 devices in a mesh: sp: 4 (over z), fs: 4 (over y, x), tp: 2 (over core).
Axes of the slice: x: 2, y: 2, z: 4, core: 2. Of those that a mesh axis runs over, the one named last changes fastest.
Arguments:
- inputs: bfloat16 [2048, 2048], P(('fs', 'sp'), 'tp'), parts along dimension 0, may hold values from -6 to 6
- norm_gain: float32 [2048], replicated, may hold values from 0.1 to 1.9
- in_ssm: bfloat16 [2048, 1024], P('sp', 'tp'), may hold values from -0.125 to 0.125
- in_query: bfloat16 [2048, 1024], P('sp', 'tp')
- in_key: bfloat16 [2048, 256], P('sp', 'tp')
- in_value: bfloat16 [2048, 256], P('sp', 'tp'), may hold values from -0.125 to 0.125
- decay_rate: float32 [64, 64], P('tp'), as said below
- rotation: float32 [64, 64], P('tp'), may hold values from 0.05 to 3
- input_parts: bfloat16 [2, 64, 64, 16], P(None, 'tp')
- output_parts: bfloat16 [2, 64, 16, 64], P(None, 'tp'), may hold values from -0.5 to 0.5
- skip_scale: float32 [64, 16], P('tp'), may hold values from -4 to 4
- decay_shift: float32 [2048, 64], P(('fs', 'sp'), 'tp'), parts along dimension 0, may hold values from -1 to 0
- sink_logit: float32 [16], P('tp'), may hold values from 2 to 6
- out_state: bfloat16 [1024, 2048], P('tp', 'sp'), may hold values from -0.125 to 0.125
- out_attend: bfloat16 [1024, 2048], P('tp', 'sp'), may hold values from -0.125 to 0.125
Outputs:
- mixed: bfloat16 [2048, 2048], P(('fs', 'sp', 'tp')), parts along dimension 0
The draws below stay inside these ranges and needn't reach their ends.
There are 4 independent parts, one for each index of `fs`. The reference program is written for one: setup_inputs(seed, part) draws one part's arguments, and reference() takes and returns one part's arrays. A program takes and returns all parts, laid end to end along the dimension named above; an argument that names none is the same for every part. Nothing has to cross between parts.
Inputs may be any that keep to these rules, and one draw needn't show every extreme that they name: `decay_rate`: between 1e-5 and 0.1.
All inputs are finite; a program needn't handle non-finite values.
Results may differ from the reference program's by a relative error of at most 0.012.
Values may be sent and summed in bfloat16 or wider, within the bound.
A program may use at most 64 MiB of HBM per device.

```python
import math
import jax
import jax.numpy as jnp
from jax import lax

D = 2048
GROUPS = 64
GROUP_CH = 16
STATE = 64
Q_HEADS = 16
KV_HEADS = 4
HEAD_DIM = 64
WINDOW = 128
BLOCK = 128
TOK_DEV = 128
LEN = 512
N_SP = 4


def recurrence_law(key):
    mask_key = jax.random.fold_in(key, 11)
    slow_key = jax.random.fold_in(key, 12)
    fast_key = jax.random.fold_in(key, 13)
    part_key = jax.random.fold_in(key, 14)
    portion = 0.5
    slow = jax.random.uniform(mask_key, (GROUPS, STATE), jnp.float32) < portion
    slow_rate = jnp.exp(jax.random.uniform(slow_key, (GROUPS, STATE), jnp.float32, math.log(0.1), math.log(0.4))) / LEN
    fast_rate = jnp.exp(jax.random.uniform(fast_key, (GROUPS, STATE), jnp.float32, math.log(0.02), math.log(0.1)))
    rates = jnp.where(slow, slow_rate, fast_rate)
    spread = jnp.sqrt(1.0 - jnp.exp(-2.0 * rates)) / math.sqrt(GROUP_CH)
    parts = jax.random.normal(part_key, (2, GROUPS, STATE, GROUP_CH), jnp.float32) * spread[None, :, :, None]
    return (rates, parts)


def draw_decay_rate(key, part):
    return recurrence_law(key)[0].astype(jnp.float32)


def draw_input_parts(key, part):
    return recurrence_law(key)[1].astype(jnp.bfloat16)


def attention_law(key):
    noise_key = jax.random.fold_in(key, 22)
    other_key = jax.random.fold_in(key, 23)
    repeat = Q_HEADS // KV_HEADS
    noise = jax.random.normal(noise_key, (D, KV_HEADS, repeat, HEAD_DIM), jnp.float32) / math.sqrt(D)
    keys_part = jax.random.normal(other_key, (D, KV_HEADS, HEAD_DIM), jnp.float32) / math.sqrt(D)
    queries_part = noise
    return (queries_part.reshape(D, Q_HEADS * HEAD_DIM), keys_part.reshape(D, KV_HEADS * HEAD_DIM))


def draw_in_query(key, part):
    return attention_law(key)[0].astype(jnp.bfloat16)


def draw_in_key(key, part):
    return attention_law(key)[1].astype(jnp.bfloat16)


def draw_decay_shift(key, part):
    factor_key = jax.random.fold_in(key, 31)
    noise_key = jax.random.fold_in(key, 32)
    place_key = jax.random.fold_in(key, 33)
    depth_key = jax.random.fold_in(key, 34)
    factor = jnp.exp(jax.random.uniform(factor_key, (LEN // TOK_DEV,), jnp.float32, math.log(0.5), math.log(2.0)))
    per_position = jnp.repeat(factor, TOK_DEV)
    rough = jax.random.uniform(noise_key, (LEN, GROUPS), jnp.float32, 0.25, 1.75)
    background = -(0.3 / LEN) * per_position[:, None] * rough
    places = jax.random.randint(place_key, (2,), 0, LEN)
    struck = jnp.any(jnp.arange(LEN, dtype=jnp.int32)[:, None] == places[None, :], axis=1)
    kept = jax.random.uniform(depth_key, (GROUPS,), jnp.float32, 0.6, 0.8)
    return (background + jnp.where(struck[:, None], jnp.log(kept)[None, :], 0.0)).astype(jnp.float32)


def level_of(rng, shape, cuts, smallest, largest):
    factor_of, own = 1.0, jax.random.fold_in(rng, 6)
    for axis_at, shards_of in cuts:
        heights = jnp.exp(jax.random.uniform(jax.random.fold_in(own, axis_at), (shards_of,), jnp.float32, smallest / len(cuts), largest / len(cuts)))
        factor_of = factor_of * jnp.repeat(heights, shape[axis_at] // shards_of).reshape([-1 if axis == axis_at else 1 for axis in range(len(shape))])
    return factor_of


def normal_values(stream_key, extent, scale, most, cuts=(), held_as=jnp.bfloat16):
    loudness = level_of(stream_key, extent, cuts, -0.22, 0.18) if cuts else 1.0
    entries = jax.random.normal(stream_key, extent, jnp.float32) * scale * loudness
    return jnp.minimum(jnp.maximum(entries, -most), most).astype(held_as)


def setup_inputs(seed: int = 0, part: int = 0) -> dict:
    key_list = jax.random.split(jax.random.key(seed), 16)
    part_keys = jax.random.split(jax.random.fold_in(key_list[15], part), 16)
    return {
        "inputs": normal_values(part_keys[0], (LEN, D), 1.0, 6.0, ((0, 4), (1, 2))),
        "norm_gain": jnp.clip(1.0 + 0.18 * jax.random.normal(key_list[1], (D,), jnp.float32), 0.1, 1.9),
        "in_ssm": normal_values(key_list[2], (D, GROUPS * GROUP_CH), D ** -0.5, 0.125, ((0, 4), (1, 2))),
        "in_query": draw_in_query(jax.random.fold_in(key_list[15], 71), part),
        "in_key": draw_in_key(jax.random.fold_in(key_list[15], 71), part),
        "in_value": normal_values(key_list[5], (D, KV_HEADS * HEAD_DIM), D ** -0.5, 0.125, ((0, 4), (1, 2))),
        "decay_rate": draw_decay_rate(jax.random.fold_in(key_list[15], 71), part),
        "rotation": jnp.clip(0.05 + 2.95 * jax.random.uniform(key_list[7], (GROUPS, STATE), jnp.float32) ** level_of(key_list[7], (GROUPS, STATE), ((0, 2),), -0.2, 0.2), 0.05, 3.0),
        "input_parts": draw_input_parts(jax.random.fold_in(key_list[15], 71), part),
        "output_parts": normal_values(key_list[9], (2, GROUPS, GROUP_CH, STATE), (2 * STATE) ** -0.5, 0.5, ((1, 2),)),
        "skip_scale": normal_values(key_list[10], (GROUPS, GROUP_CH), 1.0, 4.0, ((0, 2),), jnp.float32),
        "decay_shift": draw_decay_shift(jax.random.fold_in(jax.random.fold_in(key_list[15], part), 71), part),
        "sink_logit": jnp.clip(2.0 + 4.0 * jax.random.uniform(key_list[12], (Q_HEADS,), jnp.float32) ** level_of(key_list[12], (Q_HEADS,), ((0, 2),), -0.2, 0.2), 2.0, 6.0),
        "out_state": normal_values(key_list[13], (GROUPS * GROUP_CH, D), (GROUPS * GROUP_CH + Q_HEADS * HEAD_DIM) ** -0.5, 0.125, ((0, 2), (1, 4))),
        "out_attend": normal_values(key_list[14], (Q_HEADS * HEAD_DIM, D), (GROUPS * GROUP_CH + Q_HEADS * HEAD_DIM) ** -0.5, 0.125, ((0, 2), (1, 4))),
    }


epsilon = 1e-06
floor_score = -1e+30

def combine(earlier, later):
    first_re, first_im, state_re, state_im = earlier
    second_re, second_im, input_re, input_im = later
    return (second_re * first_re - second_im * first_im, second_re * first_im + second_im * first_re, second_re * state_re - second_im * state_im + input_re, second_re * state_im + second_im * state_re + input_im)

def input_matrix(decay_rate, rotation, input_parts):
    damped = jnp.exp(-decay_rate)
    lift_re = damped * jnp.cos(rotation) - 1.0
    lift_im = damped * jnp.sin(rotation)
    modulus = decay_rate * decay_rate + rotation * rotation
    factor_re = (rotation * lift_im - decay_rate * lift_re) / modulus
    factor_im = -(rotation * lift_re + decay_rate * lift_im) / modulus
    part_re = input_parts[0].astype(jnp.float32)
    part_im = input_parts[1].astype(jnp.float32)
    joined_re = factor_re[:, :, None] * part_re - factor_im[:, :, None] * part_im
    joined_im = factor_re[:, :, None] * part_im + factor_im[:, :, None] * part_re
    return jnp.concatenate([joined_re, joined_im], axis=1).astype(jnp.bfloat16)

def advance_block(carry, drive, shift, grouped, decay_rate, rotation, output_parts, skip_scale):
    carry_re, carry_im = carry
    width = drive.shape[2] // 2
    magnitude = jnp.exp(shift[:, :, None] - decay_rate[None])
    elements = (magnitude * jnp.cos(rotation)[None], magnitude * jnp.sin(rotation)[None], drive[:, :, :width], drive[:, :, width:])
    decay_re, decay_im, state_re, state_im = lax.associative_scan(combine, elements, axis=0)
    state_re = state_re + decay_re * carry_re[None] - decay_im * carry_im[None]
    state_im = state_im + decay_re * carry_im[None] + decay_im * carry_re[None]
    read_re = output_parts[0].astype(jnp.float32)
    read_im = output_parts[1].astype(jnp.float32)
    result = jnp.einsum('tgp,ghp->tgh', state_re, read_re, precision=lax.Precision.HIGHEST)
    result = result - jnp.einsum('tgp,ghp->tgh', state_im, read_im, precision=lax.Precision.HIGHEST)
    result = result + skip_scale.astype(jnp.float32)[None] * grouped.astype(jnp.float32)
    return ((state_re[-1], state_im[-1]), jax.nn.gelu(result).astype(jnp.bfloat16))

def window_attention(queries, keys_win, values_win, starts, sink_logit):
    window = queries.shape[1]
    scores = jnp.einsum('nqgrd,nkgd->ngrqk', queries.astype(jnp.float32), keys_win.astype(jnp.float32))
    scores = scores * queries.shape[-1] ** (-0.5)
    places = jnp.arange(window, dtype=jnp.int32)[:, None] + window - jnp.arange(2 * window, dtype=jnp.int32)[None, :]
    inside = (places >= 0) & (places < window)
    reach = starts[:, None] - window + jnp.arange(2 * window, dtype=jnp.int32)[None, :] >= 0
    valid = (inside[None] & reach[:, None, :])[:, None, None]
    sinks = sink_logit.astype(jnp.float32).reshape(scores.shape[1], scores.shape[2])[None, :, :, None, None]
    scores = jnp.where(valid, scores, floor_score)
    row_peak = jnp.maximum(lax.optimization_barrier(jnp.max(scores, axis=-1, keepdims=True)), sinks)
    raised = jnp.where(valid, jnp.exp(scores - row_peak), 0.0)
    denominator = lax.optimization_barrier(jnp.sum(raised, axis=-1, keepdims=True)) + jnp.exp(sinks - row_peak)
    weights = (raised / denominator).astype(jnp.bfloat16)
    result = jnp.einsum('ngrqk,nkgd->nqgrd', weights.astype(jnp.float32), values_win.astype(jnp.float32))
    return result.astype(jnp.bfloat16)

def reference(inputs, norm_gain, in_ssm, in_query, in_key, in_value, decay_rate, rotation, input_parts, output_parts, skip_scale, decay_shift, sink_logit, out_state, out_attend):
    length = inputs.shape[0]
    widened = inputs.astype(jnp.float32)
    scale = lax.rsqrt(lax.optimization_barrier(jnp.mean(widened * widened, axis=1, keepdims=True)) + epsilon)
    normed = (widened * scale * norm_gain.astype(jnp.float32)).astype(jnp.bfloat16)
    drive_in = jnp.dot(normed, in_ssm, preferred_element_type=jnp.float32).astype(jnp.bfloat16)
    queries = jnp.dot(normed, in_query, preferred_element_type=jnp.float32).astype(jnp.bfloat16)
    keys_local = jnp.dot(normed, in_key, preferred_element_type=jnp.float32).astype(jnp.bfloat16)
    values = jnp.dot(normed, in_value, preferred_element_type=jnp.float32).astype(jnp.bfloat16)
    in_matrix = input_matrix(decay_rate, rotation, input_parts)
    blocks = length // BLOCK
    grouped = drive_in.reshape(blocks, BLOCK, GROUPS, GROUP_CH)
    shifted = decay_shift.reshape(blocks, BLOCK, GROUPS)

    def advance(carry, pieces):
        grouped_part, shift_part = pieces
        drive = jnp.einsum('tgh,gqh->tgq', grouped_part.astype(jnp.float32), in_matrix.astype(jnp.float32))
        return advance_block(carry, drive, shift_part, grouped_part, decay_rate, rotation, output_parts, skip_scale)
    zero_state = jnp.zeros((GROUPS, STATE), jnp.float32)
    _, state_out = lax.scan(advance, (zero_state, zero_state), (grouped, shifted))
    state_out = state_out.reshape(length, GROUPS * GROUP_CH)
    windows_all = length // WINDOW
    per_device = TOK_DEV // WINDOW
    filler = jnp.zeros((WINDOW, KV_HEADS * HEAD_DIM), jnp.bfloat16)

    def windows(flat):
        split = jnp.concatenate([filler, flat], axis=0).reshape(windows_all + 1, WINDOW, KV_HEADS, HEAD_DIM)
        joined = jnp.concatenate([split[:-1], split[1:]], axis=1)
        return joined.reshape(N_SP, per_device, 2 * WINDOW, KV_HEADS, HEAD_DIM)
    queries_blk = queries.reshape(N_SP, per_device, WINDOW, KV_HEADS, Q_HEADS // KV_HEADS, HEAD_DIM)
    starts = (jnp.arange(windows_all, dtype=jnp.int32) * WINDOW).reshape(N_SP, per_device)
    attended = lax.map(lambda pieces: window_attention(pieces[0], pieces[1], pieces[2], pieces[3], sink_logit), (queries_blk, windows(keys_local), windows(values), starts))
    attend_out = attended.reshape(length, Q_HEADS * HEAD_DIM)
    summed = jnp.dot(state_out, out_state, preferred_element_type=jnp.float32)
    summed = summed + jnp.dot(attend_out, out_attend, preferred_element_type=jnp.float32)
    return summed.astype(jnp.bfloat16)
```

```python
import functools
import jax
import jax.numpy as jnp
from jax import lax
from jax.experimental import pallas as pl
from jax.experimental.pallas import tpu as pltpu
from jax.sharding import PartitionSpec as P

GROUP_CH = 16
HEAD_DIM = 64
WINDOW = 128
BLOCK = 128


epsilon = 1e-06
floor_score = -1e30


def prefix(x, axis, join, neutral):
    place = lax.axis_index(axis)
    gathered = jax.tree.map(
        lambda a, kind: lax.all_gather(a.astype(kind), axis),
        x,
        (jnp.bfloat16, jnp.bfloat16, jnp.bfloat16, jnp.bfloat16),
    )
    state = jax.tree.map(lambda a, e: jnp.zeros_like(a) + jnp.asarray(e, a.dtype), x, neutral)

    def one(hop, state):
        return join(
            state,
            jax.tree.map(
                lambda a, own: lax.dynamic_index_in_dim(a, hop, 0, False).astype(own.dtype),
                gathered,
                x,
            ),
        )

    return lax.fori_loop(0, place, one, state)


def from_behind(value, axis, steps):
    count = lax.axis_size(axis)
    initial, last = (max(0, -steps), min(count, count - steps))
    return lax.ppermute(value, axis, [(source, source + steps) for source in range(initial, last)])


def combine(earlier, later):
    first_re, first_im, state_re, state_im = earlier
    second_re, second_im, input_re, input_im = later
    return (
        second_re * first_re - second_im * first_im,
        second_re * first_im + second_im * first_re,
        second_re * state_re - second_im * state_im + input_re,
        second_re * state_im + second_im * state_re + input_im,
    )


def input_matrix(decay_rate, rotation, input_parts):
    damped = jnp.exp(-decay_rate)
    lift_re = damped * jnp.cos(rotation) - 1.0
    lift_im = damped * jnp.sin(rotation)
    modulus = decay_rate * decay_rate + rotation * rotation
    factor_re = (rotation * lift_im - decay_rate * lift_re) / modulus
    factor_im = -(rotation * lift_re + decay_rate * lift_im) / modulus
    part_re = input_parts[0].astype(jnp.float32)
    part_im = input_parts[1].astype(jnp.float32)
    joined_re = factor_re[:, :, None] * part_re - factor_im[:, :, None] * part_im
    joined_im = factor_re[:, :, None] * part_im + factor_im[:, :, None] * part_re
    return jnp.concatenate([joined_re, joined_im], axis=1).astype(jnp.bfloat16)


def window_attention(queries, keys_win, values_win, starts, sink_logit):
    window = queries.shape[1]
    scores = jnp.einsum("nqgrd,nkgd->ngrqk", queries, keys_win, preferred_element_type=jnp.float32)
    scores = scores * queries.shape[-1] ** (-0.5)
    places = (
        jnp.arange(window, dtype=jnp.int32)[:, None]
        + window
        - jnp.arange(2 * window, dtype=jnp.int32)[None, :]
    )
    inside = (places >= 0) & (places < window)
    reach = starts[:, None] - window + jnp.arange(2 * window, dtype=jnp.int32)[None, :] >= 0
    valid = (inside[None] & reach[:, None, :])[:, None, None]
    sinks = sink_logit.reshape(scores.shape[1], scores.shape[2])[None, :, :, None, None]
    scores = jnp.where(valid, scores, floor_score)
    row_peak = jnp.maximum(jnp.max(scores, axis=-1, keepdims=True), sinks)
    raised = jnp.where(valid, jnp.exp(scores - row_peak), 0.0)
    denominator = jnp.sum(raised, axis=-1, keepdims=True) + jnp.exp(sinks - row_peak)
    weights = (raised / denominator).astype(jnp.bfloat16)
    result = jnp.einsum(
        "ngrqk,nkgd->nqgrd", weights, values_win, preferred_element_type=jnp.float32
    )
    return result.astype(jnp.bfloat16)


def general_body(
    inputs,
    norm_gain,
    in_ssm,
    in_query,
    in_key,
    in_value,
    decay_rate,
    rotation,
    input_parts,
    output_parts,
    skip_scale,
    decay_shift,
    sink_logit,
    out_state,
    out_attend,
):
    gathered = lax.all_gather(inputs, "tp", axis=1, tiled=True)
    length = gathered.shape[0]
    widened = gathered.astype(jnp.float32)
    scale = lax.rsqrt(jnp.mean(widened * widened, axis=1, keepdims=True) + epsilon)
    normed = (widened * scale * norm_gain).astype(jnp.bfloat16)

    def add_rows(pieces):
        return tuple(
            (jnp.dot(normed, piece, preferred_element_type=jnp.float32) for piece in pieces)
        )

    projected = add_rows(
        (
            lax.all_gather(in_ssm, "sp", axis=0, tiled=True),
            lax.all_gather(in_query, "sp", axis=0, tiled=True),
            lax.all_gather(in_key, "sp", axis=0, tiled=True),
            lax.all_gather(in_value, "sp", axis=0, tiled=True),
        )
    )
    drive_in, queries, keys_local, values = [piece.astype(jnp.bfloat16) for piece in projected]
    groups = decay_rate.shape[0]
    state_dim = decay_rate.shape[1]
    channels = groups * GROUP_CH
    highest = lax.Precision.HIGHEST
    drive_cols = jnp.transpose(drive_in).reshape(groups, GROUP_CH, length)
    in_matrix = input_matrix(decay_rate, rotation, input_parts)
    drive = jnp.einsum("gqh,ght->gqt", in_matrix, drive_cols, preferred_element_type=jnp.float32)
    shift_cols = jnp.transpose(decay_shift)
    running = jnp.cumsum(shift_cols, axis=1)
    total_shift = running[:, -1]
    remain = length - 1.0 - jnp.arange(length, dtype=jnp.float32)
    to_end = (total_shift[:, None] - running)[:, None, :] - decay_rate[:, :, None] * remain[
        None, None, :
    ]
    fade = jnp.exp(to_end)
    turn = rotation[:, :, None] * remain[None, None, :]
    weight_re = fade * jnp.cos(turn)
    weight_im = fade * jnp.sin(turn)
    drive_re = drive[:, :state_dim]
    drive_im = drive[:, state_dim:]
    final_re = jnp.sum(weight_re * drive_re - weight_im * drive_im, axis=2)
    final_im = jnp.sum(weight_re * drive_im + weight_im * drive_re, axis=2)
    overall = jnp.exp(total_shift[:, None] - decay_rate * length)
    nothing = jnp.zeros_like(final_re)
    carried = prefix(
        (
            overall * jnp.cos(rotation * length),
            overall * jnp.sin(rotation * length),
            final_re,
            final_im,
        ),
        "sp",
        combine,
        (jnp.ones_like(final_re), nothing, nothing, nothing),
    )
    key_heads = keys_local.shape[1] // HEAD_DIM
    query_heads = queries.shape[1] // HEAD_DIM
    windows_dev = length // WINDOW
    previous = from_behind((keys_local, values), "sp", 1)

    def windows(flat, before):
        split = jnp.concatenate([before, flat], axis=0).reshape(
            windows_dev + 1, WINDOW, key_heads, HEAD_DIM
        )
        return jnp.concatenate([split[:-1], split[1:]], axis=1)

    offset = lax.axis_index("sp") * length
    starts = offset + jnp.arange(windows_dev, dtype=jnp.int32) * WINDOW
    queries_blk = queries.reshape(
        windows_dev, WINDOW, key_heads, query_heads // key_heads, HEAD_DIM
    )
    attended = window_attention(
        queries_blk,
        windows(keys_local, previous[0]),
        windows(values, previous[1]),
        starts,
        sink_logit,
    )
    attend_out = attended.reshape(length, query_heads * HEAD_DIM)
    blocks = length // BLOCK
    triangle = (
        jnp.arange(BLOCK, dtype=jnp.int32)[:, None] <= jnp.arange(BLOCK, dtype=jnp.int32)[None, :]
    ).astype(jnp.float32)
    offsets = jnp.arange(BLOCK, dtype=jnp.float32)
    centre = BLOCK // 2
    read_re = output_parts[0].astype(jnp.float32)
    read_im = output_parts[1].astype(jnp.float32)
    angle = rotation[:, :, None] * (offsets - centre)[None, None, :]
    cos_angle = jnp.cos(angle)
    sin_angle = jnp.sin(angle)
    phase = rotation[:, :, None] * (offsets + 1.0)[None, None, :]
    cos_phase = jnp.cos(phase)
    sin_phase = jnp.sin(phase)

    def advance(carry, pieces):
        carry_re, carry_im = carry
        part_re, part_im, shift_part, grouped_part = pieces
        level = jnp.dot(shift_part, triangle, precision=highest)
        log_from = level[:, None, :] - decay_rate[:, :, None] * (offsets + 1.0)[None, None, :]
        relative = log_from - log_from[:, :, centre : centre + 1]
        shrink = jnp.exp(-relative)
        lift_re = shrink * (part_re * cos_angle + part_im * sin_angle)
        lift_im = shrink * (part_im * cos_angle - part_re * sin_angle)
        prefix_re = jnp.dot(lift_re.reshape(groups * state_dim, BLOCK), triangle, precision=highest)
        prefix_im = jnp.dot(lift_im.reshape(groups * state_dim, BLOCK), triangle, precision=highest)
        prefix_re = prefix_re.reshape(groups, state_dim, BLOCK)
        prefix_im = prefix_im.reshape(groups, state_dim, BLOCK)
        grow = jnp.exp(relative)
        from_start = jnp.exp(log_from)
        keep_re = from_start * cos_phase
        keep_im = from_start * sin_phase
        state_re = grow * (prefix_re * cos_angle - prefix_im * sin_angle)
        state_im = grow * (prefix_im * cos_angle + prefix_re * sin_angle)
        state_re = state_re + keep_re * carry_re[:, :, None] - keep_im * carry_im[:, :, None]
        state_im = state_im + keep_re * carry_im[:, :, None] + keep_im * carry_re[:, :, None]
        result = jnp.einsum("ghp,gpt->ght", read_re, state_re, precision=highest)
        result = result - jnp.einsum("ghp,gpt->ght", read_im, state_im, precision=highest)
        result = result + skip_scale[:, :, None] * grouped_part.astype(jnp.float32)
        return ((state_re[:, :, -1], state_im[:, :, -1]), jax.nn.gelu(result).astype(jnp.bfloat16))

    drive_blocks = jnp.transpose(drive.reshape(groups, 2 * state_dim, blocks, BLOCK), (2, 0, 1, 3))
    shift_blocks = jnp.transpose(shift_cols.reshape(groups, blocks, BLOCK), (1, 0, 2))
    grouped_blocks = jnp.transpose(
        drive_cols.reshape(groups, GROUP_CH, blocks, BLOCK), (2, 0, 1, 3)
    )
    _, state_blocks = lax.scan(
        advance,
        (carried[2], carried[3]),
        (
            drive_blocks[:, :, :state_dim],
            drive_blocks[:, :, state_dim:],
            shift_blocks,
            grouped_blocks,
        ),
    )
    state_out = jnp.transpose(state_blocks, (0, 3, 1, 2)).reshape(length, channels)
    column_state, column_attend = (
        lax.all_gather(out_state, "sp", axis=1, tiled=True),
        lax.all_gather(out_attend, "sp", axis=1, tiled=True),
    )
    result = jnp.dot(state_out, column_state, preferred_element_type=jnp.float32)
    return lax.psum_scatter(
        (result + jnp.dot(attend_out, column_attend, preferred_element_type=jnp.float32)).astype(
            jnp.bfloat16
        ),
        "tp",
        scatter_dimension=0,
        tiled=True,
    )


MESH = pl.DeviceIdType.MESH
ANY = pl.BlockSpec(memory_space=pl.ANY)


def remote(src, dst, send, recv, **where):
    return pltpu.make_async_remote_copy(
        src_ref=src, dst_ref=dst, send_sem=send, recv_sem=recv, device_id=where, device_id_type=MESH
    )


def greet(peers):
    barrier = pltpu.get_barrier_semaphore()
    for peer in peers:
        pl.semaphore_signal(barrier, inc=1, device_id=peer, device_id_type=MESH)
    pl.semaphore_wait(barrier, len(peers))


def spread_kernel(n, n_fs, n_tp, repeat_dev, x, ssm, query, kv, shift, ows, owa,
                  xg, w_ssm, w_query, w_kv, shift_g, ows_g, owa_g,
                  held_x, held_w, held_s, held_o, held_p,
                  x_send, x_recv, xp_send, xp_recv, w_send, w_recv, f_send, f_recv,
                  s_send, s_recv, o_send, o_recv, in_sem, out_sem):
    k = lax.axis_index("sp")
    f = lax.axis_index("fs")
    t = lax.axis_index("tp")
    tokens, half = x.shape
    rows = ssm.shape[0]
    part = rows // n_fs
    cs, cq = w_ssm.shape[1], w_query.shape[1]
    groups = shift_g.shape[0]
    other = 1 - t
    peers = [{"sp": lax.rem(k + s, n)} for s in range(1, n)]
    peers += [{"fs": lax.rem(f + d, n_fs)} for d in range(1, n_fs)]
    peers += [{"tp": other}]
    greet(peers)
    order = sorted(range(1, n), key=lambda s: -min(s, n - s))

    def piece(which, place, span):
        if which == 0:
            return ssm.at[span, pl.ds(pl.multiple_of(place * cs, 128), cs)]
        if which == 1:
            return query.at[span, pl.ds(pl.multiple_of(place * cq, 128), cq)]
        return kv.at[lax.div(place, repeat_dev), span]

    dests = (w_ssm, w_query, w_kv)

    def x_at(j, side):
        return xg.at[pl.ds(pl.multiple_of(j * tokens, 128), tokens),
                     pl.ds(pl.multiple_of(side * half, 128), half)]

    copies = []
    for s in order:
        peer = lax.rem(k + s, n)
        for which in range(3):
            mine = pl.ds(pl.multiple_of(f * part, 16), part)
            into = pl.ds(pl.multiple_of(k * rows + f * part, 16), part)
            copies.append(remote(piece(which, peer, mine), dests[which].at[into],
                                 w_send.at[which, s - 1], w_recv.at[which, s - 1], sp=peer))
            copies[-1].start()
    partner = [remote(x, x_at(k, t), xp_send.at[0], xp_recv.at[0], tp=other)]
    partner[0].start()
    x_copies = {}
    for s in order:
        peer = lax.rem(k + s, n)
        x_copies[s] = remote(x, x_at(k, t), x_send.at[s - 1], x_recv.at[s - 1], sp=peer)
        x_copies[s].start()
        c = remote(shift.at[pl.ds(pl.multiple_of(peer * groups, 8), groups)],
                   shift_g.at[:, pl.ds(pl.multiple_of(k * tokens, 128), tokens)],
                   s_send.at[s - 1], s_recv.at[s - 1], sp=peer)
        c.start()
        copies.append(c)
    o_rows = pl.ds(pl.multiple_of(t * ows.shape[0], 16), ows.shape[0])
    for i, (src, dst) in enumerate(((ows, ows_g), (owa, owa_g))):
        c = remote(src, dst.at[o_rows], o_send.at[i], o_recv.at[i], tp=other)
        c.start()
        copies.append(c)
    everything = pl.ds(0, rows)
    here = pl.ds(pl.multiple_of(k * rows, 16), rows)
    local = [(x, held_x, x_at(k, t))]
    for which in range(3):
        local.append((piece(which, k, everything), held_w.at[which], dests[which].at[here]))
    local.append((shift.at[pl.ds(pl.multiple_of(k * groups, 8), groups)], held_s,
                  shift_g.at[:, pl.ds(pl.multiple_of(k * tokens, 128), tokens)]))
    local.append((ows, held_o, ows_g.at[o_rows]))
    local.append((owa, held_p, owa_g.at[o_rows]))
    ins = [pltpu.make_async_copy(a, b, in_sem.at[i]) for i, (a, b, _) in enumerate(local)]
    outs = [pltpu.make_async_copy(b, c, out_sem.at[i]) for i, (_, b, c) in enumerate(local)]
    for c in ins:
        c.start()
    for a, b in zip(ins, outs):
        a.wait()
        b.start()
    forwards = []
    for i, s in enumerate(sorted(range(1, n), key=lambda s: min(s, n - s))):
        source = lax.rem(k + n - s, n)
        into = pl.ds(pl.multiple_of(source * rows + f * part, 16), part)
        for which in range(3):
            got = dests[which].at[into]
            remote(got, got, w_send.at[which, s - 1], w_recv.at[which, s - 1], sp=source).wait_recv()
            for d in range(1, n_fs):
                c = remote(got, got, f_send.at[which, s - 1, d - 1], f_recv.at[which, s - 1, d - 1],
                           fs=lax.rem(f + d, n_fs))
                c.start()
                forwards.append(c)
    for s in sorted(range(1, n), key=lambda s: min(s, n - s)):
        x_copies[s].wait_recv()
        block = x_at(lax.rem(k + n - s, n), t)
        c = remote(block, block, xp_send.at[s], xp_recv.at[s], tp=other)
        c.start()
        partner.append(c)
    for c in copies:
        c.wait_send()
    for c in copies[3 * (n - 1):]:
        c.wait_recv()
    for c in x_copies.values():
        c.wait_send()
    for c in partner + forwards:
        c.wait()
    for c in outs:
        c.wait()


def spread(n, n_fs, n_tp, repeat_dev, x, ssm, query, kv, shift, ows, owa):
    tokens, half = x.shape
    rows = ssm.shape[0]
    cs, cq, ck = ssm.shape[1] // n, query.shape[1] // n, kv.shape[2]
    groups = shift.shape[0] // n
    bf = jnp.bfloat16
    dma = pltpu.SemaphoreType.DMA
    return pl.pallas_call(
        functools.partial(spread_kernel, n, n_fs, n_tp, repeat_dev),
        out_shape=[
            jax.ShapeDtypeStruct((n * tokens, n_tp * half), bf),
            jax.ShapeDtypeStruct((n * rows, cs), bf),
            jax.ShapeDtypeStruct((n * rows, cq), bf),
            jax.ShapeDtypeStruct((n * rows, ck), bf),
            jax.ShapeDtypeStruct((groups, n * tokens), jnp.float32),
            jax.ShapeDtypeStruct((n_tp * ows.shape[0], ows.shape[1]), bf),
            jax.ShapeDtypeStruct((n_tp * owa.shape[0], owa.shape[1]), bf),
        ],
        in_specs=[ANY] * 7,
        out_specs=[ANY] * 7,
        scratch_shapes=[
            pltpu.VMEM(x.shape, bf),
            pltpu.VMEM((3, rows, cs), bf),
            pltpu.VMEM((groups, tokens), jnp.float32),
            pltpu.VMEM(ows.shape, bf),
            pltpu.VMEM(owa.shape, bf),
            dma((n - 1,)), dma((n - 1,)), dma((n,)), dma((n,)),
            dma((3, n - 1)), dma((3, n - 1)),
            dma((3, n - 1, n_fs - 1)), dma((3, n - 1, n_fs - 1)),
            dma((n - 1,)), dma((n - 1,)), dma((2,)), dma((2,)), dma((7,)), dma((7,)),
        ],
        compiler_params=pltpu.CompilerParams(collective_id=0, has_side_effects=True),
    )(x, ssm, query, kv, shift, ows, owa)


def join_kernel(n, hs, ha, gs, ga, held, send, recv, in_sem, out_sem):
    k = lax.axis_index("sp")
    t = lax.axis_index("tp")
    width = hs.shape[2]
    pairs = [(s, r) for s in range(n) for r in range(2) if (s, r) != (0, 0)]
    pairs = sorted(pairs, key=lambda p: -min(p[0], n - p[0]))
    greet([{"sp": lax.rem(k + s, n), "tp": lax.rem(t + r, 2)} for s, r in pairs])
    columns = pl.ds(pl.multiple_of((t * n + k) * width, 128), width)
    copies = []
    for s, r in pairs:
        for i, (src, dst) in enumerate(((hs, gs), (ha, ga))):
            side = lax.rem(t + r, 2)
            c = remote(src.at[side], dst.at[:, columns], send.at[i, s, r], recv.at[i, s, r],
                       sp=lax.rem(k + s, n), tp=side)
            c.start()
            copies.append(c)
    for i, (src, dst) in enumerate(((hs, gs), (ha, ga))):
        c = pltpu.make_async_copy(src.at[t], held.at[i], in_sem.at[i])
        c.start()
        c.wait()
        c = pltpu.make_async_copy(held.at[i], dst.at[:, columns], out_sem.at[i])
        c.start()
        c.wait()
    for c in copies:
        c.wait()


def join(n, hs, ha):
    _, rows, width = hs.shape
    dma = pltpu.SemaphoreType.DMA
    return pl.pallas_call(
        functools.partial(join_kernel, n),
        out_shape=[jax.ShapeDtypeStruct((rows, 2 * n * width), jnp.bfloat16)] * 2,
        in_specs=[ANY] * 2,
        out_specs=[ANY] * 2,
        scratch_shapes=[pltpu.VMEM((2, rows, width), jnp.bfloat16),
                        dma((2, n, 2)), dma((2, n, 2)), dma((2,)), dma((2,))],
        compiler_params=pltpu.CompilerParams(collective_id=1, has_side_effects=True),
    )(hs, ha)


def settle_kernel(n, src, out, held, send, recv, in_sem, out_sem):
    k = lax.axis_index("sp")
    rows, width = src.shape[0] // n, src.shape[1]
    order = sorted(range(1, n), key=lambda s: -min(s, n - s))
    greet([{"sp": lax.rem(k + s, n)} for s in order])
    columns = pl.ds(pl.multiple_of(k * width, 128), width)
    copies = []
    for s in order:
        peer = lax.rem(k + s, n)
        c = remote(src.at[pl.ds(pl.multiple_of(peer * rows, 16), rows)], out.at[:, columns],
                   send.at[s], recv.at[s], sp=peer)
        c.start()
        copies.append(c)
    c = pltpu.make_async_copy(src.at[pl.ds(pl.multiple_of(k * rows, 16), rows)], held, in_sem.at[0])
    c.start()
    c.wait()
    c = pltpu.make_async_copy(held, out.at[:, columns], out_sem.at[0])
    c.start()
    c.wait()
    for c in copies:
        c.wait()


def settle(n, mixed):
    rows, width = mixed.shape[0] // n, mixed.shape[1]
    dma = pltpu.SemaphoreType.DMA
    return pl.pallas_call(
        functools.partial(settle_kernel, n),
        out_shape=jax.ShapeDtypeStruct((rows, n * width), jnp.bfloat16),
        in_specs=[ANY],
        out_specs=ANY,
        scratch_shapes=[pltpu.VMEM((rows, width), jnp.bfloat16), dma((n,)), dma((n,)), dma((1,)), dma((1,))],
        compiler_params=pltpu.CompilerParams(collective_id=2, has_side_effects=True),
    )(mixed)


def recurrence(drive_in, shift_cols, decay_rate, rotation, input_parts, output_parts, skip_scale):
    length = drive_in.shape[0]
    groups, state_dim = decay_rate.shape
    highest = lax.Precision.HIGHEST
    drive_cols = jnp.transpose(drive_in).reshape(groups, GROUP_CH, length)
    in_matrix = input_matrix(decay_rate, rotation, input_parts)
    drive = jnp.einsum("gqh,ght->gqt", in_matrix, drive_cols, preferred_element_type=jnp.float32)
    blocks = length // BLOCK
    triangle = (
        jnp.arange(BLOCK, dtype=jnp.int32)[:, None] <= jnp.arange(BLOCK, dtype=jnp.int32)[None, :]
    ).astype(jnp.float32)
    offsets = jnp.arange(BLOCK, dtype=jnp.float32)
    centre = BLOCK // 2
    read_re = output_parts[0].astype(jnp.float32)
    read_im = output_parts[1].astype(jnp.float32)
    angle = rotation[:, :, None] * (offsets - centre)[None, None, :]
    cos_angle = jnp.cos(angle)
    sin_angle = jnp.sin(angle)
    phase = rotation[:, :, None] * (offsets + 1.0)[None, None, :]
    cos_phase = jnp.cos(phase)
    sin_phase = jnp.sin(phase)
    carry_re = jnp.zeros((groups, state_dim), jnp.float32)
    carry_im = carry_re
    results = []
    for block in range(blocks):
        span = slice(block * BLOCK, (block + 1) * BLOCK)
        part_re = drive[:, :state_dim, span]
        part_im = drive[:, state_dim:, span]
        level = jnp.dot(shift_cols[:, span], triangle, precision=highest)
        log_from = level[:, None, :] - decay_rate[:, :, None] * (offsets + 1.0)[None, None, :]
        relative = log_from - log_from[:, :, centre : centre + 1]
        shrink = jnp.exp(-relative)
        lift_re = shrink * (part_re * cos_angle + part_im * sin_angle)
        lift_im = shrink * (part_im * cos_angle - part_re * sin_angle)
        prefix_re = jnp.dot(lift_re.reshape(groups * state_dim, BLOCK), triangle, precision=highest)
        prefix_im = jnp.dot(lift_im.reshape(groups * state_dim, BLOCK), triangle, precision=highest)
        prefix_re = prefix_re.reshape(groups, state_dim, BLOCK)
        prefix_im = prefix_im.reshape(groups, state_dim, BLOCK)
        grow = jnp.exp(relative)
        from_start = jnp.exp(log_from)
        keep_re = from_start * cos_phase
        keep_im = from_start * sin_phase
        state_re = grow * (prefix_re * cos_angle - prefix_im * sin_angle)
        state_im = grow * (prefix_im * cos_angle + prefix_re * sin_angle)
        state_re = state_re + keep_re * carry_re[:, :, None] - keep_im * carry_im[:, :, None]
        state_im = state_im + keep_re * carry_im[:, :, None] + keep_im * carry_re[:, :, None]
        result = jnp.einsum("ghp,gpt->ght", read_re, state_re, precision=highest)
        result = result - jnp.einsum("ghp,gpt->ght", read_im, state_im, precision=highest)
        result = result + skip_scale[:, :, None] * drive_cols[:, :, span].astype(jnp.float32)
        carry_re, carry_im = state_re[:, :, -1], state_im[:, :, -1]
        results.append(jax.nn.gelu(result).astype(jnp.bfloat16))
    return jnp.transpose(jnp.concatenate(results, axis=2).reshape(groups * GROUP_CH, length))


def fast_body(
    inputs, norm_gain, in_ssm, in_query, in_key, in_value, decay_rate, rotation, input_parts,
    output_parts, skip_scale, decay_shift, sink_logit, out_state, out_attend,
):
    n, n_fs, n_tp = lax.axis_size("sp"), lax.axis_size("fs"), lax.axis_size("tp")
    k = lax.axis_index("sp")
    key_heads = in_key.shape[1] // HEAD_DIM
    query_heads = in_query.shape[1] // HEAD_DIM
    heads = query_heads // n
    rows = in_key.shape[0]
    kv = jnp.concatenate(
        [in_key.reshape(rows, key_heads, HEAD_DIM), in_value.reshape(rows, key_heads, HEAD_DIM)], axis=2
    ).transpose(1, 0, 2)
    gathered, w_ssm, w_query, w_kv, shift_cols, ows, owa = spread(
        n, n_fs, n_tp, n // key_heads, inputs, in_ssm, in_query, kv,
        jnp.transpose(decay_shift), out_state, out_attend,
    )
    length = gathered.shape[0]
    widened = gathered.astype(jnp.float32)
    scale = lax.rsqrt(jnp.mean(widened * widened, axis=1, keepdims=True) + epsilon)
    normed = (widened * scale * norm_gain).astype(jnp.bfloat16)
    drive_in, queries, kv_cols = [
        jnp.dot(normed, w, preferred_element_type=jnp.float32).astype(jnp.bfloat16)
        for w in (w_ssm, w_query, w_kv)
    ]

    def own(array, axis):
        size = array.shape[axis] // n
        return lax.dynamic_slice_in_dim(array, k * size, size, axis)

    state_out = recurrence(
        drive_in, shift_cols, own(decay_rate, 0), own(rotation, 0), own(input_parts, 1),
        own(output_parts, 1), own(skip_scale, 0),
    )
    count = length // WINDOW

    def windows(flat):
        split = jnp.concatenate([jnp.zeros((WINDOW, HEAD_DIM), flat.dtype), flat], axis=0)
        split = split.reshape(count + 1, WINDOW, 1, HEAD_DIM)
        return jnp.concatenate([split[:-1], split[1:]], axis=1)

    attended = window_attention(
        queries.reshape(count, WINDOW, 1, heads, HEAD_DIM),
        windows(kv_cols[:, :HEAD_DIM]),
        windows(kv_cols[:, HEAD_DIM:]),
        jnp.arange(count, dtype=jnp.int32) * WINDOW,
        own(sink_logit, 0),
    )
    attend_out = attended.reshape(length, heads * HEAD_DIM)
    tokens = length // n

    def by_side(flat):
        split = flat.reshape(n, n_tp, tokens // n_tp, flat.shape[1])
        return split.transpose(1, 0, 2, 3).reshape(n_tp, length // n_tp, flat.shape[1])

    all_state, all_attend = join(n, by_side(state_out), by_side(attend_out))
    result = jnp.dot(all_state, ows, preferred_element_type=jnp.float32)
    result = result + jnp.dot(all_attend, owa, preferred_element_type=jnp.float32)
    return settle(n, result.astype(jnp.bfloat16))


def body(*args):
    n, n_fs, n_tp = lax.axis_size("sp"), lax.axis_size("fs"), lax.axis_size("tp")
    inputs, in_ssm, in_query, in_key, decay_rate = args[0], args[2], args[3], args[4], args[6]
    key_heads = in_key.shape[1] // HEAD_DIM
    query_heads = in_query.shape[1] // HEAD_DIM
    fits = (
        n_tp == 2
        and 1 < n <= 8
        and n_fs > 1
        and n % key_heads == 0
        and query_heads % n == 0
        and in_ssm.shape[1] == in_query.shape[1]
        and in_ssm.shape[1] % (128 * n) == 0
        and 2 * HEAD_DIM == in_ssm.shape[1] // n
        and decay_rate.shape[0] % (8 * n) == 0
        and decay_rate.shape[0] * GROUP_CH == in_ssm.shape[1]
        and inputs.shape[0] % 128 == 0
        and inputs.shape[1] % 128 == 0
        and in_ssm.shape[0] % (16 * n_fs) == 0
        and args[13].shape[1] % 128 == 0
    )
    return (fast_body if fits else general_body)(*args)


def solution(mesh):
    return jax.shard_map(
        body,
        mesh=mesh,
        in_specs=(
            P(("fs", "sp"), "tp"),
            P(),
            P("sp", "tp"),
            P("sp", "tp"),
            P("sp", "tp"),
            P("sp", "tp"),
            P("tp", None),
            P("tp", None),
            P(None, "tp", None, None),
            P(None, "tp", None, None),
            P("tp", None),
            P(("fs", "sp"), "tp"),
            P("tp"),
            P("tp", "sp"),
            P("tp", "sp"),
        ),
        out_specs=P(("fs", "sp", "tp"), None),
        check_vma=False,
    )
```

```python
import functools
import jax
import jax.numpy as jnp
from jax import lax
from jax.experimental import pallas as pl
from jax.experimental.pallas import tpu as pltpu
from jax.sharding import PartitionSpec as P

GROUP_CH = 16
HEAD_DIM = 64
WINDOW = 128
BLOCK = 128


epsilon = 1e-06
floor_score = -1e30


def prefix(x, axis, join, neutral):
    place = lax.axis_index(axis)
    gathered = jax.tree.map(
        lambda a, kind: lax.all_gather(a.astype(kind), axis),
        x,
        (jnp.bfloat16, jnp.bfloat16, jnp.bfloat16, jnp.bfloat16),
    )
    state = jax.tree.map(lambda a, e: jnp.zeros_like(a) + jnp.asarray(e, a.dtype), x, neutral)

    def one(hop, state):
        return join(
            state,
            jax.tree.map(
                lambda a, own: lax.dynamic_index_in_dim(a, hop, 0, False).astype(own.dtype),
                gathered,
                x,
            ),
        )

    return lax.fori_loop(0, place, one, state)


def from_behind(value, axis, steps):
    count = lax.axis_size(axis)
    initial, last = (max(0, -steps), min(count, count - steps))
    return lax.ppermute(value, axis, [(source, source + steps) for source in range(initial, last)])


def combine(earlier, later):
    first_re, first_im, state_re, state_im = earlier
    second_re, second_im, input_re, input_im = later
    return (
        second_re * first_re - second_im * first_im,
        second_re * first_im + second_im * first_re,
        second_re * state_re - second_im * state_im + input_re,
        second_re * state_im + second_im * state_re + input_im,
    )


def input_matrix(decay_rate, rotation, input_parts):
    damped = jnp.exp(-decay_rate)
    lift_re = damped * jnp.cos(rotation) - 1.0
    lift_im = damped * jnp.sin(rotation)
    modulus = decay_rate * decay_rate + rotation * rotation
    factor_re = (rotation * lift_im - decay_rate * lift_re) / modulus
    factor_im = -(rotation * lift_re + decay_rate * lift_im) / modulus
    part_re = input_parts[0].astype(jnp.float32)
    part_im = input_parts[1].astype(jnp.float32)
    joined_re = factor_re[:, :, None] * part_re - factor_im[:, :, None] * part_im
    joined_im = factor_re[:, :, None] * part_im + factor_im[:, :, None] * part_re
    return jnp.concatenate([joined_re, joined_im], axis=1).astype(jnp.bfloat16)


def window_attention(queries, keys_win, values_win, starts, sink_logit):
    window = queries.shape[1]
    scores = jnp.einsum("nqgrd,nkgd->ngrqk", queries, keys_win, preferred_element_type=jnp.float32)
    scores = scores * queries.shape[-1] ** (-0.5)
    places = (
        jnp.arange(window, dtype=jnp.int32)[:, None]
        + window
        - jnp.arange(2 * window, dtype=jnp.int32)[None, :]
    )
    inside = (places >= 0) & (places < window)
    reach = starts[:, None] - window + jnp.arange(2 * window, dtype=jnp.int32)[None, :] >= 0
    valid = (inside[None] & reach[:, None, :])[:, None, None]
    sinks = sink_logit.reshape(scores.shape[1], scores.shape[2])[None, :, :, None, None]
    scores = jnp.where(valid, scores, floor_score)
    row_peak = jnp.maximum(jnp.max(scores, axis=-1, keepdims=True), sinks)
    raised = jnp.where(valid, jnp.exp(scores - row_peak), 0.0)
    denominator = jnp.sum(raised, axis=-1, keepdims=True) + jnp.exp(sinks - row_peak)
    weights = (raised / denominator).astype(jnp.bfloat16)
    result = jnp.einsum(
        "ngrqk,nkgd->nqgrd", weights, values_win, preferred_element_type=jnp.float32
    )
    return result.astype(jnp.bfloat16)


def general_body(
    inputs,
    norm_gain,
    in_ssm,
    in_query,
    in_key,
    in_value,
    decay_rate,
    rotation,
    input_parts,
    output_parts,
    skip_scale,
    decay_shift,
    sink_logit,
    out_state,
    out_attend,
):
    gathered = lax.all_gather(inputs, "tp", axis=1, tiled=True)
    length = gathered.shape[0]
    widened = gathered.astype(jnp.float32)
    scale = lax.rsqrt(jnp.mean(widened * widened, axis=1, keepdims=True) + epsilon)
    normed = (widened * scale * norm_gain).astype(jnp.bfloat16)

    def add_rows(pieces):
        return tuple(
            (jnp.dot(normed, piece, preferred_element_type=jnp.float32) for piece in pieces)
        )

    projected = add_rows(
        (
            lax.all_gather(in_ssm, "sp", axis=0, tiled=True),
            lax.all_gather(in_query, "sp", axis=0, tiled=True),
            lax.all_gather(in_key, "sp", axis=0, tiled=True),
            lax.all_gather(in_value, "sp", axis=0, tiled=True),
        )
    )
    drive_in, queries, keys_local, values = [piece.astype(jnp.bfloat16) for piece in projected]
    groups = decay_rate.shape[0]
    state_dim = decay_rate.shape[1]
    channels = groups * GROUP_CH
    highest = lax.Precision.HIGHEST
    drive_cols = jnp.transpose(drive_in).reshape(groups, GROUP_CH, length)
    in_matrix = input_matrix(decay_rate, rotation, input_parts)
    drive = jnp.einsum("gqh,ght->gqt", in_matrix, drive_cols, preferred_element_type=jnp.float32)
    shift_cols = jnp.transpose(decay_shift)
    running = jnp.cumsum(shift_cols, axis=1)
    total_shift = running[:, -1]
    remain = length - 1.0 - jnp.arange(length, dtype=jnp.float32)
    to_end = (total_shift[:, None] - running)[:, None, :] - decay_rate[:, :, None] * remain[
        None, None, :
    ]
    fade = jnp.exp(to_end)
    turn = rotation[:, :, None] * remain[None, None, :]
    weight_re = fade * jnp.cos(turn)
    weight_im = fade * jnp.sin(turn)
    drive_re = drive[:, :state_dim]
    drive_im = drive[:, state_dim:]
    final_re = jnp.sum(weight_re * drive_re - weight_im * drive_im, axis=2)
    final_im = jnp.sum(weight_re * drive_im + weight_im * drive_re, axis=2)
    overall = jnp.exp(total_shift[:, None] - decay_rate * length)
    nothing = jnp.zeros_like(final_re)
    carried = prefix(
        (
            overall * jnp.cos(rotation * length),
            overall * jnp.sin(rotation * length),
            final_re,
            final_im,
        ),
        "sp",
        combine,
        (jnp.ones_like(final_re), nothing, nothing, nothing),
    )
    key_heads = keys_local.shape[1] // HEAD_DIM
    query_heads = queries.shape[1] // HEAD_DIM
    windows_dev = length // WINDOW
    previous = from_behind((keys_local, values), "sp", 1)

    def windows(flat, before):
        split = jnp.concatenate([before, flat], axis=0).reshape(
            windows_dev + 1, WINDOW, key_heads, HEAD_DIM
        )
        return jnp.concatenate([split[:-1], split[1:]], axis=1)

    offset = lax.axis_index("sp") * length
    starts = offset + jnp.arange(windows_dev, dtype=jnp.int32) * WINDOW
    queries_blk = queries.reshape(
        windows_dev, WINDOW, key_heads, query_heads // key_heads, HEAD_DIM
    )
    attended = window_attention(
        queries_blk,
        windows(keys_local, previous[0]),
        windows(values, previous[1]),
        starts,
        sink_logit,
    )
    attend_out = attended.reshape(length, query_heads * HEAD_DIM)
    blocks = length // BLOCK
    triangle = (
        jnp.arange(BLOCK, dtype=jnp.int32)[:, None] <= jnp.arange(BLOCK, dtype=jnp.int32)[None, :]
    ).astype(jnp.float32)
    offsets = jnp.arange(BLOCK, dtype=jnp.float32)
    centre = BLOCK // 2
    read_re = output_parts[0].astype(jnp.float32)
    read_im = output_parts[1].astype(jnp.float32)
    angle = rotation[:, :, None] * (offsets - centre)[None, None, :]
    cos_angle = jnp.cos(angle)
    sin_angle = jnp.sin(angle)
    phase = rotation[:, :, None] * (offsets + 1.0)[None, None, :]
    cos_phase = jnp.cos(phase)
    sin_phase = jnp.sin(phase)

    def advance(carry, pieces):
        carry_re, carry_im = carry
        part_re, part_im, shift_part, grouped_part = pieces
        level = jnp.dot(shift_part, triangle, precision=highest)
        log_from = level[:, None, :] - decay_rate[:, :, None] * (offsets + 1.0)[None, None, :]
        relative = log_from - log_from[:, :, centre : centre + 1]
        shrink = jnp.exp(-relative)
        lift_re = shrink * (part_re * cos_angle + part_im * sin_angle)
        lift_im = shrink * (part_im * cos_angle - part_re * sin_angle)
        prefix_re = jnp.dot(lift_re.reshape(groups * state_dim, BLOCK), triangle, precision=highest)
        prefix_im = jnp.dot(lift_im.reshape(groups * state_dim, BLOCK), triangle, precision=highest)
        prefix_re = prefix_re.reshape(groups, state_dim, BLOCK)
        prefix_im = prefix_im.reshape(groups, state_dim, BLOCK)
        grow = jnp.exp(relative)
        from_start = jnp.exp(log_from)
        keep_re = from_start * cos_phase
        keep_im = from_start * sin_phase
        state_re = grow * (prefix_re * cos_angle - prefix_im * sin_angle)
        state_im = grow * (prefix_im * cos_angle + prefix_re * sin_angle)
        state_re = state_re + keep_re * carry_re[:, :, None] - keep_im * carry_im[:, :, None]
        state_im = state_im + keep_re * carry_im[:, :, None] + keep_im * carry_re[:, :, None]
        result = jnp.einsum("ghp,gpt->ght", read_re, state_re, precision=highest)
        result = result - jnp.einsum("ghp,gpt->ght", read_im, state_im, precision=highest)
        result = result + skip_scale[:, :, None] * grouped_part.astype(jnp.float32)
        return ((state_re[:, :, -1], state_im[:, :, -1]), jax.nn.gelu(result).astype(jnp.bfloat16))

    drive_blocks = jnp.transpose(drive.reshape(groups, 2 * state_dim, blocks, BLOCK), (2, 0, 1, 3))
    shift_blocks = jnp.transpose(shift_cols.reshape(groups, blocks, BLOCK), (1, 0, 2))
    grouped_blocks = jnp.transpose(
        drive_cols.reshape(groups, GROUP_CH, blocks, BLOCK), (2, 0, 1, 3)
    )
    _, state_blocks = lax.scan(
        advance,
        (carried[2], carried[3]),
        (
            drive_blocks[:, :, :state_dim],
            drive_blocks[:, :, state_dim:],
            shift_blocks,
            grouped_blocks,
        ),
    )
    state_out = jnp.transpose(state_blocks, (0, 3, 1, 2)).reshape(length, channels)
    column_state, column_attend = (
        lax.all_gather(out_state, "sp", axis=1, tiled=True),
        lax.all_gather(out_attend, "sp", axis=1, tiled=True),
    )
    result = jnp.dot(state_out, column_state, preferred_element_type=jnp.float32)
    return lax.psum_scatter(
        (result + jnp.dot(attend_out, column_attend, preferred_element_type=jnp.float32)).astype(
            jnp.bfloat16
        ),
        "tp",
        scatter_dimension=0,
        tiled=True,
    )


MESH = pl.DeviceIdType.MESH
ANY = pl.BlockSpec(memory_space=pl.ANY)


def remote(src, dst, send, recv, **where):
    return pltpu.make_async_remote_copy(
        src_ref=src, dst_ref=dst, send_sem=send, recv_sem=recv, device_id=where, device_id_type=MESH
    )


def greet(peers):
    barrier = pltpu.get_barrier_semaphore()
    for peer in peers:
        pl.semaphore_signal(barrier, inc=1, device_id=peer, device_id_type=MESH)
    pl.semaphore_wait(barrier, len(peers))


def spread_kernel(n, n_fs, n_tp, repeat_dev, x, ssm, query, kv, shift, ows, owa,
                  xg, w_ssm, w_query, w_kv, shift_g, ows_g, owa_g,
                  held_x, held_w, held_s, held_o, held_p,
                  x_send, x_recv, q_send, q_recv, xp_send, xp_recv, w_send, w_recv, f_send, f_recv,
                  s_send, s_recv, o_send, o_recv, in_sem, out_sem):
    k = lax.axis_index("sp")
    f = lax.axis_index("fs")
    t = lax.axis_index("tp")
    tokens, half = x.shape
    rows = ssm.shape[0]
    part = rows // n_fs
    cs, cq = w_ssm.shape[1], w_query.shape[1]
    groups = shift_g.shape[0]
    other = 1 - t
    peers = [{"sp": lax.rem(k + s, n)} for s in range(1, n)]
    peers += [{"fs": lax.rem(f + d, n_fs)} for d in range(1, n_fs)]
    peers += [{"tp": other}]
    greet(peers)
    order = sorted(range(1, n), key=lambda s: -min(s, n - s))

    def piece(which, place, span):
        if which == 0:
            return ssm.at[span, pl.ds(pl.multiple_of(place * cs, 128), cs)]
        if which == 1:
            return query.at[span, pl.ds(pl.multiple_of(place * cq, 128), cq)]
        return kv.at[lax.div(place, repeat_dev), span]

    dests = (w_ssm, w_query, w_kv)

    def x_at(j, side):
        return xg.at[pl.ds(pl.multiple_of(j * tokens, 128), tokens),
                     pl.ds(pl.multiple_of(side * half, 128), half)]

    copies = []
    for s in order:
        peer = lax.rem(k + s, n)
        for which in range(3):
            mine = pl.ds(pl.multiple_of(f * part, 16), part)
            into = pl.ds(pl.multiple_of(k * rows + f * part, 16), part)
            copies.append(remote(piece(which, peer, mine), dests[which].at[into],
                                 w_send.at[which, s - 1], w_recv.at[which, s - 1], sp=peer))
            copies[-1].start()
    partner = [remote(x, x_at(k, t), xp_send.at[0], xp_recv.at[0], tp=other)]
    partner[0].start()
    for s in order:
        peer = lax.rem(k + s, n)
        c = remote(shift.at[pl.ds(pl.multiple_of(peer * groups, 8), groups)],
                   shift_g.at[:, pl.ds(pl.multiple_of(k * tokens, 128), tokens)],
                   s_send.at[s - 1], s_recv.at[s - 1], sp=peer)
        c.start()
        copies.append(c)

    def hop(step, way):
        block = lax.rem(k - way * step + n, n)
        dst = x_at(block, t)
        src = x if step == 0 else dst
        to = lax.rem(k + way + n, n)
        i = 0 if way > 0 else 1
        active = jnp.logical_and(k + way >= 0, k + way < n)
        active = jnp.logical_and(active, jnp.logical_and(k - way * step >= 0, k - way * step < n))
        return active, remote(src, dst, x_send.at[i, step], x_recv.at[i, step], sp=to)

    def arrival(step, way):
        origin = k - way * (step + 1)
        block = x_at(lax.rem(origin + n, n), t)
        i = 0 if way > 0 else 1
        active = jnp.logical_and(origin >= 0, origin < n)
        c = remote(block, block, x_send.at[i, step], x_recv.at[i, step], sp=lax.rem(k - way + n, n))
        p = remote(block, block, q_send.at[i, step], q_recv.at[i, step], tp=other)
        return active, c, p

    def start_hops(step):
        for way in (1, -1):
            active, c = hop(step, way)

            @pl.when(active)
            def _():
                c.start()

    start_hops(0)
    o_rows = pl.ds(pl.multiple_of(t * ows.shape[0], 16), ows.shape[0])
    for i, (src, dst) in enumerate(((ows, ows_g), (owa, owa_g))):
        c = remote(src, dst.at[o_rows], o_send.at[i], o_recv.at[i], tp=other)
        c.start()
        copies.append(c)
    everything = pl.ds(0, rows)
    here = pl.ds(pl.multiple_of(k * rows, 16), rows)
    local = [(x, held_x, x_at(k, t))]
    for which in range(3):
        local.append((piece(which, k, everything), held_w.at[which], dests[which].at[here]))
    local.append((shift.at[pl.ds(pl.multiple_of(k * groups, 8), groups)], held_s,
                  shift_g.at[:, pl.ds(pl.multiple_of(k * tokens, 128), tokens)]))
    local.append((ows, held_o, ows_g.at[o_rows]))
    local.append((owa, held_p, owa_g.at[o_rows]))
    ins = [pltpu.make_async_copy(a, b, in_sem.at[i]) for i, (a, b, _) in enumerate(local)]
    outs = [pltpu.make_async_copy(b, c, out_sem.at[i]) for i, (_, b, c) in enumerate(local)]
    for c in ins:
        c.start()
    for a, b in zip(ins, outs):
        a.wait()
        b.start()
    forwards = []
    for i, s in enumerate(sorted(range(1, n), key=lambda s: min(s, n - s))):
        source = lax.rem(k + n - s, n)
        into = pl.ds(pl.multiple_of(source * rows + f * part, 16), part)
        for which in range(3):
            got = dests[which].at[into]
            remote(got, got, w_send.at[which, s - 1], w_recv.at[which, s - 1], sp=source).wait_recv()
            for d in range(1, n_fs):
                c = remote(got, got, f_send.at[which, s - 1, d - 1], f_recv.at[which, s - 1, d - 1],
                           fs=lax.rem(f + d, n_fs))
                c.start()
                forwards.append(c)
    for step in range(n - 1):
        for way in (1, -1):
            active, c, p = arrival(step, way)

            @pl.when(active)
            def _():
                c.wait_recv()
                p.start()

        if step + 1 < n - 1:
            start_hops(step + 1)
    for step in range(n - 1):
        for way in (1, -1):
            active, c = hop(step, way)

            @pl.when(active)
            def _():
                c.wait_send()

            active, _c, p = arrival(step, way)

            @pl.when(active)
            def _():
                p.wait()

    for c in copies:
        c.wait_send()
    for c in copies[3 * (n - 1):]:
        c.wait_recv()
    for c in partner + forwards:
        c.wait()
    for c in outs:
        c.wait()


def spread(n, n_fs, n_tp, repeat_dev, x, ssm, query, kv, shift, ows, owa):
    tokens, half = x.shape
    rows = ssm.shape[0]
    cs, cq, ck = ssm.shape[1] // n, query.shape[1] // n, kv.shape[2]
    groups = shift.shape[0] // n
    bf = jnp.bfloat16
    dma = pltpu.SemaphoreType.DMA
    return pl.pallas_call(
        functools.partial(spread_kernel, n, n_fs, n_tp, repeat_dev),
        out_shape=[
            jax.ShapeDtypeStruct((n * tokens, n_tp * half), bf),
            jax.ShapeDtypeStruct((n * rows, cs), bf),
            jax.ShapeDtypeStruct((n * rows, cq), bf),
            jax.ShapeDtypeStruct((n * rows, ck), bf),
            jax.ShapeDtypeStruct((groups, n * tokens), jnp.float32),
            jax.ShapeDtypeStruct((n_tp * ows.shape[0], ows.shape[1]), bf),
            jax.ShapeDtypeStruct((n_tp * owa.shape[0], owa.shape[1]), bf),
        ],
        in_specs=[ANY] * 7,
        out_specs=[ANY] * 7,
        scratch_shapes=[
            pltpu.VMEM(x.shape, bf),
            pltpu.VMEM((3, rows, cs), bf),
            pltpu.VMEM((groups, tokens), jnp.float32),
            pltpu.VMEM(ows.shape, bf),
            pltpu.VMEM(owa.shape, bf),
            dma((2, n - 1)), dma((2, n - 1)), dma((2, n - 1)), dma((2, n - 1)), dma((1,)), dma((1,)),
            dma((3, n - 1)), dma((3, n - 1)),
            dma((3, n - 1, n_fs - 1)), dma((3, n - 1, n_fs - 1)),
            dma((n - 1,)), dma((n - 1,)), dma((2,)), dma((2,)), dma((7,)), dma((7,)),
        ],
        compiler_params=pltpu.CompilerParams(collective_id=0, has_side_effects=True),
    )(x, ssm, query, kv, shift, ows, owa)


def join_kernel(n, hs, ha, gs, ga, held, send, recv, in_sem, out_sem):
    k = lax.axis_index("sp")
    t = lax.axis_index("tp")
    width = hs.shape[2]
    pairs = [(s, r) for s in range(n) for r in range(2) if (s, r) != (0, 0)]
    pairs = sorted(pairs, key=lambda p: -min(p[0], n - p[0]))
    greet([{"sp": lax.rem(k + s, n), "tp": lax.rem(t + r, 2)} for s, r in pairs])
    columns = pl.ds(pl.multiple_of((t * n + k) * width, 128), width)
    copies = []
    for s, r in pairs:
        for i, (src, dst) in enumerate(((hs, gs), (ha, ga))):
            side = lax.rem(t + r, 2)
            c = remote(src.at[side], dst.at[:, columns], send.at[i, s, r], recv.at[i, s, r],
                       sp=lax.rem(k + s, n), tp=side)
            c.start()
            copies.append(c)
    for i, (src, dst) in enumerate(((hs, gs), (ha, ga))):
        c = pltpu.make_async_copy(src.at[t], held.at[i], in_sem.at[i])
        c.start()
        c.wait()
        c = pltpu.make_async_copy(held.at[i], dst.at[:, columns], out_sem.at[i])
        c.start()
        c.wait()
    for c in copies:
        c.wait()


def join(n, hs, ha):
    _, rows, width = hs.shape
    dma = pltpu.SemaphoreType.DMA
    return pl.pallas_call(
        functools.partial(join_kernel, n),
        out_shape=[jax.ShapeDtypeStruct((rows, 2 * n * width), jnp.bfloat16)] * 2,
        in_specs=[ANY] * 2,
        out_specs=[ANY] * 2,
        scratch_shapes=[pltpu.VMEM((2, rows, width), jnp.bfloat16),
                        dma((2, n, 2)), dma((2, n, 2)), dma((2,)), dma((2,))],
        compiler_params=pltpu.CompilerParams(collective_id=1, has_side_effects=True),
    )(hs, ha)


def settle_kernel(n, src, out, held, send, recv, in_sem, out_sem):
    k = lax.axis_index("sp")
    rows, width = src.shape[0] // n, src.shape[1]
    order = sorted(range(1, n), key=lambda s: -min(s, n - s))
    greet([{"sp": lax.rem(k + s, n)} for s in order])
    columns = pl.ds(pl.multiple_of(k * width, 128), width)
    copies = []
    for s in order:
        peer = lax.rem(k + s, n)
        c = remote(src.at[pl.ds(pl.multiple_of(peer * rows, 16), rows)], out.at[:, columns],
                   send.at[s], recv.at[s], sp=peer)
        c.start()
        copies.append(c)
    c = pltpu.make_async_copy(src.at[pl.ds(pl.multiple_of(k * rows, 16), rows)], held, in_sem.at[0])
    c.start()
    c.wait()
    c = pltpu.make_async_copy(held, out.at[:, columns], out_sem.at[0])
    c.start()
    c.wait()
    for c in copies:
        c.wait()


def settle(n, mixed):
    rows, width = mixed.shape[0] // n, mixed.shape[1]
    dma = pltpu.SemaphoreType.DMA
    return pl.pallas_call(
        functools.partial(settle_kernel, n),
        out_shape=jax.ShapeDtypeStruct((rows, n * width), jnp.bfloat16),
        in_specs=[ANY],
        out_specs=ANY,
        scratch_shapes=[pltpu.VMEM((rows, width), jnp.bfloat16), dma((n,)), dma((n,)), dma((1,)), dma((1,))],
        compiler_params=pltpu.CompilerParams(collective_id=2, has_side_effects=True),
    )(mixed)


def halves(x):
    high = x.astype(jnp.bfloat16)
    return high, (x - high.astype(jnp.float32)).astype(jnp.bfloat16)


def split_dot(x, exact):
    high, low = halves(x)
    return jnp.dot(high, exact, preferred_element_type=jnp.float32) + jnp.dot(
        low, exact, preferred_element_type=jnp.float32
    )


def column(row):
    size = row.shape[1]
    same = lax.broadcasted_iota(jnp.int32, (size, size), 0) == lax.broadcasted_iota(
        jnp.int32, (size, size), 1
    )
    return jnp.sum(jnp.where(same, row, 0.0), axis=1, keepdims=True)


def mixer_kernel(k, x, gain, w_ssm, w_query, w_kv, shift, rate, rotation, in_parts, out_parts,
                 skip, sinks, hs, ha, u_scr, q_scr, kv_scr, y_scr):
    f32, bf = jnp.float32, jnp.bfloat16
    length = x.shape[0]
    blocks = length // BLOCK
    groups = shift.shape[0]
    state = rate.shape[1]
    heads = w_query.shape[1] // HEAD_DIM
    side = BLOCK // 2
    kv_scr[0:WINDOW, :] = jnp.zeros((WINDOW, kv_scr.shape[1]), bf)

    for b in range(blocks):
        span = slice(b * BLOCK, (b + 1) * BLOCK)
        wide = x[span, :].astype(f32)
        scale = lax.rsqrt(jnp.mean(wide * wide, axis=1, keepdims=True) + epsilon)
        normed = (wide * scale * gain[...]).astype(bf)
        u = jnp.dot(normed, w_ssm[...], preferred_element_type=f32)
        u_scr[:, span] = jnp.transpose(u.astype(bf).astype(f32))
        q_scr[span, :] = jnp.dot(normed, w_query[...], preferred_element_type=f32).astype(bf)
        kv_scr[(b + 1) * BLOCK : (b + 2) * BLOCK, :] = jnp.dot(
            normed, w_kv[...], preferred_element_type=f32
        ).astype(bf)

    shape = (BLOCK, BLOCK)
    upto = lax.broadcasted_iota(jnp.int32, shape, 0) <= lax.broadcasted_iota(jnp.int32, shape, 1)
    tri = upto.astype(f32).astype(bf)
    centre = BLOCK // 2
    levels, lifts, grows, starts = [], [], [], []
    for b in range(blocks):
        part = shift[:, b * BLOCK : (b + 1) * BLOCK]
        high, low = halves(part)
        low2 = (part - high.astype(f32) - low.astype(f32)).astype(bf)
        level = (
            jnp.dot(high, tri, preferred_element_type=f32)
            + jnp.dot(low, tri, preferred_element_type=f32)
            + jnp.dot(low2, tri, preferred_element_type=f32)
        )
        middle = level[:, centre : centre + 1]
        lifts.append(jnp.exp(middle - level))
        grows.append(jnp.exp(level - middle))
        starts.append(jnp.exp(middle))
    away = lax.broadcasted_iota(jnp.int32, (state, BLOCK), 1).astype(f32) - float(centre)
    first = k * groups
    for g in range(groups):
        rates = column(rate[pl.ds(first + g, 1), :])
        turns = column(rotation[pl.ds(first + g, 1), :])
        angle = turns * away
        cos, sin = jnp.cos(angle), jnp.sin(angle)
        fade = jnp.exp(-rates * away)
        rise = jnp.exp(rates * away)
        up_re, up_im = rise * cos, -(rise * sin)
        down_re, down_im = fade * cos, fade * sin
        damped = jnp.exp(-rates)
        lift_re = damped * jnp.cos(turns) - 1.0
        lift_im = damped * jnp.sin(turns)
        modulus = rates * rates + turns * turns
        factor_re = (turns * lift_im - rates * lift_re) / modulus
        factor_im = -(turns * lift_re + rates * lift_im) / modulus
        part_re = in_parts[0, first + g].astype(f32)
        part_im = in_parts[1, first + g].astype(f32)
        in_matrix = jnp.concatenate(
            [factor_re * part_re - factor_im * part_im, factor_re * part_im + factor_im * part_re],
            axis=0,
        ).astype(bf)
        read = jnp.concatenate(
            [out_parts[0, first + g].astype(f32), -out_parts[1, first + g].astype(f32)], axis=1
        ).astype(bf)
        reach = jnp.exp(-rates * (centre + 1.0))
        reach_re = reach * jnp.cos(turns * (centre + 1.0))
        reach_im = reach * jnp.sin(turns * (centre + 1.0))
        u = u_scr[g * GROUP_CH : (g + 1) * GROUP_CH, :]
        drive = jnp.dot(in_matrix, u.astype(bf), preferred_element_type=f32)
        lifted = []
        for b in range(blocks):
            span = slice(b * BLOCK, (b + 1) * BLOCK)
            row = lifts[b][g : g + 1, :]
            d_re, d_im = drive[:state, span] * row, drive[state:, span] * row
            lifted += [d_re * up_re - d_im * up_im, d_re * up_im + d_im * up_re]
        prefix = split_dot(jnp.concatenate(lifted, axis=0), tri)
        carry_re = jnp.zeros((state, 1), f32)
        carry_im = carry_re
        skips = column(skip[pl.ds(first + g, 1), :])
        for b in range(blocks):
            span = slice(b * BLOCK, (b + 1) * BLOCK)
            begin = starts[b][g : g + 1, :]
            base_re = begin * (carry_re * reach_re - carry_im * reach_im)
            base_im = begin * (carry_re * reach_im + carry_im * reach_re)
            p_re = prefix[2 * b * state : (2 * b + 1) * state] + base_re
            p_im = prefix[(2 * b + 1) * state : (2 * b + 2) * state] + base_im
            row = grows[b][g : g + 1, :]
            s_re = row * (down_re * p_re - down_im * p_im)
            s_im = row * (down_re * p_im + down_im * p_re)
            carry_re, carry_im = s_re[:, BLOCK - 1 :], s_im[:, BLOCK - 1 :]
            high, low = halves(jnp.concatenate([s_re, s_im], axis=0))
            y = jnp.dot(read, high, preferred_element_type=f32) + jnp.dot(
                read, low, preferred_element_type=f32
            )
            y_scr[g * GROUP_CH : (g + 1) * GROUP_CH, span] = y + skips * u[:, span]

    for b in range(blocks):
        y = y_scr[:, b * BLOCK : (b + 1) * BLOCK]
        y = jnp.transpose(jax.nn.gelu(y)).astype(bf)
        hs[0, b * side : (b + 1) * side, :] = y[:side]
        hs[1, b * side : (b + 1) * side, :] = y[side:]

    wide = (WINDOW, 2 * WINDOW)
    gap = lax.broadcasted_iota(jnp.int32, wide, 0) + WINDOW - lax.broadcasted_iota(jnp.int32, wide, 1)
    inside = (gap >= 0) & (gap < WINDOW)
    inside_first = inside & (lax.broadcasted_iota(jnp.int32, wide, 1) >= WINDOW)
    for b in range(blocks):
        keys = kv_scr[b * WINDOW : (b + 2) * WINDOW, :HEAD_DIM]
        values = kv_scr[b * WINDOW : (b + 2) * WINDOW, HEAD_DIM:]
        valid = inside if b else inside_first
        outs = []
        for h in range(heads):
            query = q_scr[b * WINDOW : (b + 1) * WINDOW, h * HEAD_DIM : (h + 1) * HEAD_DIM]
            scores = lax.dot_general(query, keys, (((1,), (1,)), ((), ())), preferred_element_type=f32)
            scores = jnp.where(valid, scores * HEAD_DIM ** (-0.5), floor_score)
            sink = sinks[k * heads + h]
            peak = jnp.maximum(jnp.max(scores, axis=1, keepdims=True), sink)
            raised = jnp.where(valid, jnp.exp(scores - peak), 0.0)
            total = jnp.sum(raised, axis=1, keepdims=True) + jnp.exp(sink - peak)
            weights = (raised / total).astype(bf)
            outs.append(jnp.dot(weights, values, preferred_element_type=f32))
        out = jnp.concatenate(outs, axis=1).astype(bf)
        ha[0, b * side : (b + 1) * side, :] = out[:side]
        ha[1, b * side : (b + 1) * side, :] = out[side:]


def mixer_entry(*refs):
    mixer_kernel(lax.axis_index("sp"), *refs)


def mixer(x, gain, w_ssm, w_query, w_kv, shift, rate, rotation, in_parts, out_parts, skip, sinks,
          entry=mixer_entry, interpret=False):
    length = x.shape[0]
    vmem = pl.BlockSpec(memory_space=pltpu.VMEM)
    return pl.pallas_call(
        entry,
        out_shape=[
            jax.ShapeDtypeStruct((2, length // 2, w_ssm.shape[1]), jnp.bfloat16),
            jax.ShapeDtypeStruct((2, length // 2, w_query.shape[1]), jnp.bfloat16),
        ],
        in_specs=[vmem] * 11 + [pl.BlockSpec(memory_space=pltpu.SMEM)],
        out_specs=[vmem] * 2,
        scratch_shapes=[
            pltpu.VMEM((w_ssm.shape[1], length), jnp.float32),
            pltpu.VMEM((length, w_query.shape[1]), jnp.bfloat16),
            pltpu.VMEM((length + WINDOW, w_kv.shape[1]), jnp.bfloat16),
            pltpu.VMEM((w_ssm.shape[1], length), jnp.float32),
        ],
        interpret=interpret,
    )(x, gain, w_ssm, w_query, w_kv, shift, rate, rotation, in_parts, out_parts, skip, sinks)


def fast_body(
    inputs, norm_gain, in_ssm, in_query, in_key, in_value, decay_rate, rotation, input_parts,
    output_parts, skip_scale, decay_shift, sink_logit, out_state, out_attend,
):
    n, n_fs, n_tp = lax.axis_size("sp"), lax.axis_size("fs"), lax.axis_size("tp")
    key_heads = in_key.shape[1] // HEAD_DIM
    rows = in_key.shape[0]
    kv = jnp.concatenate(
        [in_key.reshape(rows, key_heads, HEAD_DIM), in_value.reshape(rows, key_heads, HEAD_DIM)], axis=2
    ).transpose(1, 0, 2)
    gathered, w_ssm, w_query, w_kv, shift_cols, ows, owa = spread(
        n, n_fs, n_tp, n // key_heads, inputs, in_ssm, in_query, kv,
        jnp.transpose(decay_shift), out_state, out_attend,
    )
    by_side_state, by_side_attend = mixer(
        gathered, norm_gain[None], w_ssm, w_query, w_kv, shift_cols, decay_rate, rotation,
        input_parts, output_parts, skip_scale, sink_logit,
    )
    all_state, all_attend = join(n, by_side_state, by_side_attend)
    result = jnp.dot(all_state, ows, preferred_element_type=jnp.float32)
    result = result + jnp.dot(all_attend, owa, preferred_element_type=jnp.float32)
    return settle(n, result.astype(jnp.bfloat16))


def body(*args):
    n, n_fs, n_tp = lax.axis_size("sp"), lax.axis_size("fs"), lax.axis_size("tp")
    inputs, in_ssm, in_query, in_key, decay_rate = args[0], args[2], args[3], args[4], args[6]
    key_heads = in_key.shape[1] // HEAD_DIM
    query_heads = in_query.shape[1] // HEAD_DIM
    fits = (
        n_tp == 2
        and 1 < n <= 8
        and n_fs > 1
        and n % key_heads == 0
        and query_heads % n == 0
        and in_ssm.shape[1] == in_query.shape[1]
        and in_ssm.shape[1] % (128 * n) == 0
        and 2 * HEAD_DIM == in_ssm.shape[1] // n
        and decay_rate.shape[0] % (8 * n) == 0
        and decay_rate.shape[0] * GROUP_CH == in_ssm.shape[1]
        and inputs.shape[0] == BLOCK == WINDOW
        and inputs.shape[1] % 128 == 0
        and in_ssm.shape[0] % (16 * n_fs) == 0
        and args[13].shape[1] % 128 == 0
    )
    return (fast_body if fits else general_body)(*args)


def solution(mesh):
    return jax.shard_map(
        body,
        mesh=mesh,
        in_specs=(
            P(("fs", "sp"), "tp"),
            P(),
            P("sp", "tp"),
            P("sp", "tp"),
            P("sp", "tp"),
            P("sp", "tp"),
            P("tp", None),
            P("tp", None),
            P(None, "tp", None, None),
            P(None, "tp", None, None),
            P("tp", None),
            P(("fs", "sp"), "tp"),
            P("tp"),
            P("tp", "sp"),
            P("tp", "sp"),
        ),
        out_specs=P(("fs", "sp", "tp"), None),
        check_vma=False,
    )
```

```python
import functools
import jax
import jax.numpy as jnp
from jax import lax
from jax.experimental import pallas as pl
from jax.experimental.pallas import tpu as pltpu
from jax.sharding import PartitionSpec as P

GROUP_CH = 16
HEAD_DIM = 64
WINDOW = 128
BLOCK = 128


epsilon = 1e-06
floor_score = -1e30


def prefix(x, axis, join, neutral):
    place = lax.axis_index(axis)
    gathered = jax.tree.map(
        lambda a, kind: lax.all_gather(a.astype(kind), axis),
        x,
        (jnp.bfloat16, jnp.bfloat16, jnp.bfloat16, jnp.bfloat16),
    )
    state = jax.tree.map(lambda a, e: jnp.zeros_like(a) + jnp.asarray(e, a.dtype), x, neutral)

    def one(hop, state):
        return join(
            state,
            jax.tree.map(
                lambda a, own: lax.dynamic_index_in_dim(a, hop, 0, False).astype(own.dtype),
                gathered,
                x,
            ),
        )

    return lax.fori_loop(0, place, one, state)


def from_behind(value, axis, steps):
    count = lax.axis_size(axis)
    initial, last = (max(0, -steps), min(count, count - steps))
    return lax.ppermute(value, axis, [(source, source + steps) for source in range(initial, last)])


def combine(earlier, later):
    first_re, first_im, state_re, state_im = earlier
    second_re, second_im, input_re, input_im = later
    return (
        second_re * first_re - second_im * first_im,
        second_re * first_im + second_im * first_re,
        second_re * state_re - second_im * state_im + input_re,
        second_re * state_im + second_im * state_re + input_im,
    )


def input_matrix(decay_rate, rotation, input_parts):
    damped = jnp.exp(-decay_rate)
    lift_re = damped * jnp.cos(rotation) - 1.0
    lift_im = damped * jnp.sin(rotation)
    modulus = decay_rate * decay_rate + rotation * rotation
    factor_re = (rotation * lift_im - decay_rate * lift_re) / modulus
    factor_im = -(rotation * lift_re + decay_rate * lift_im) / modulus
    part_re = input_parts[0].astype(jnp.float32)
    part_im = input_parts[1].astype(jnp.float32)
    joined_re = factor_re[:, :, None] * part_re - factor_im[:, :, None] * part_im
    joined_im = factor_re[:, :, None] * part_im + factor_im[:, :, None] * part_re
    return jnp.concatenate([joined_re, joined_im], axis=1).astype(jnp.bfloat16)


def window_attention(queries, keys_win, values_win, starts, sink_logit):
    window = queries.shape[1]
    scores = jnp.einsum("nqgrd,nkgd->ngrqk", queries, keys_win, preferred_element_type=jnp.float32)
    scores = scores * queries.shape[-1] ** (-0.5)
    places = (
        jnp.arange(window, dtype=jnp.int32)[:, None]
        + window
        - jnp.arange(2 * window, dtype=jnp.int32)[None, :]
    )
    inside = (places >= 0) & (places < window)
    reach = starts[:, None] - window + jnp.arange(2 * window, dtype=jnp.int32)[None, :] >= 0
    valid = (inside[None] & reach[:, None, :])[:, None, None]
    sinks = sink_logit.reshape(scores.shape[1], scores.shape[2])[None, :, :, None, None]
    scores = jnp.where(valid, scores, floor_score)
    row_peak = jnp.maximum(jnp.max(scores, axis=-1, keepdims=True), sinks)
    raised = jnp.where(valid, jnp.exp(scores - row_peak), 0.0)
    denominator = jnp.sum(raised, axis=-1, keepdims=True) + jnp.exp(sinks - row_peak)
    weights = (raised / denominator).astype(jnp.bfloat16)
    result = jnp.einsum(
        "ngrqk,nkgd->nqgrd", weights, values_win, preferred_element_type=jnp.float32
    )
    return result.astype(jnp.bfloat16)


def general_body(
    inputs,
    norm_gain,
    in_ssm,
    in_query,
    in_key,
    in_value,
    decay_rate,
    rotation,
    input_parts,
    output_parts,
    skip_scale,
    decay_shift,
    sink_logit,
    out_state,
    out_attend,
):
    gathered = lax.all_gather(inputs, "tp", axis=1, tiled=True)
    length = gathered.shape[0]
    widened = gathered.astype(jnp.float32)
    scale = lax.rsqrt(jnp.mean(widened * widened, axis=1, keepdims=True) + epsilon)
    normed = (widened * scale * norm_gain).astype(jnp.bfloat16)

    def add_rows(pieces):
        return tuple(
            (jnp.dot(normed, piece, preferred_element_type=jnp.float32) for piece in pieces)
        )

    projected = add_rows(
        (
            lax.all_gather(in_ssm, "sp", axis=0, tiled=True),
            lax.all_gather(in_query, "sp", axis=0, tiled=True),
            lax.all_gather(in_key, "sp", axis=0, tiled=True),
            lax.all_gather(in_value, "sp", axis=0, tiled=True),
        )
    )
    drive_in, queries, keys_local, values = [piece.astype(jnp.bfloat16) for piece in projected]
    groups = decay_rate.shape[0]
    state_dim = decay_rate.shape[1]
    channels = groups * GROUP_CH
    highest = lax.Precision.HIGHEST
    drive_cols = jnp.transpose(drive_in).reshape(groups, GROUP_CH, length)
    in_matrix = input_matrix(decay_rate, rotation, input_parts)
    drive = jnp.einsum("gqh,ght->gqt", in_matrix, drive_cols, preferred_element_type=jnp.float32)
    shift_cols = jnp.transpose(decay_shift)
    running = jnp.cumsum(shift_cols, axis=1)
    total_shift = running[:, -1]
    remain = length - 1.0 - jnp.arange(length, dtype=jnp.float32)
    to_end = (total_shift[:, None] - running)[:, None, :] - decay_rate[:, :, None] * remain[
        None, None, :
    ]
    fade = jnp.exp(to_end)
    turn = rotation[:, :, None] * remain[None, None, :]
    weight_re = fade * jnp.cos(turn)
    weight_im = fade * jnp.sin(turn)
    drive_re = drive[:, :state_dim]
    drive_im = drive[:, state_dim:]
    final_re = jnp.sum(weight_re * drive_re - weight_im * drive_im, axis=2)
    final_im = jnp.sum(weight_re * drive_im + weight_im * drive_re, axis=2)
    overall = jnp.exp(total_shift[:, None] - decay_rate * length)
    nothing = jnp.zeros_like(final_re)
    carried = prefix(
        (
            overall * jnp.cos(rotation * length),
            overall * jnp.sin(rotation * length),
            final_re,
            final_im,
        ),
        "sp",
        combine,
        (jnp.ones_like(final_re), nothing, nothing, nothing),
    )
    key_heads = keys_local.shape[1] // HEAD_DIM
    query_heads = queries.shape[1] // HEAD_DIM
    windows_dev = length // WINDOW
    previous = from_behind((keys_local, values), "sp", 1)

    def windows(flat, before):
        split = jnp.concatenate([before, flat], axis=0).reshape(
            windows_dev + 1, WINDOW, key_heads, HEAD_DIM
        )
        return jnp.concatenate([split[:-1], split[1:]], axis=1)

    offset = lax.axis_index("sp") * length
    starts = offset + jnp.arange(windows_dev, dtype=jnp.int32) * WINDOW
    queries_blk = queries.reshape(
        windows_dev, WINDOW, key_heads, query_heads // key_heads, HEAD_DIM
    )
    attended = window_attention(
        queries_blk,
        windows(keys_local, previous[0]),
        windows(values, previous[1]),
        starts,
        sink_logit,
    )
    attend_out = attended.reshape(length, query_heads * HEAD_DIM)
    blocks = length // BLOCK
    triangle = (
        jnp.arange(BLOCK, dtype=jnp.int32)[:, None] <= jnp.arange(BLOCK, dtype=jnp.int32)[None, :]
    ).astype(jnp.float32)
    offsets = jnp.arange(BLOCK, dtype=jnp.float32)
    centre = BLOCK // 2
    read_re = output_parts[0].astype(jnp.float32)
    read_im = output_parts[1].astype(jnp.float32)
    angle = rotation[:, :, None] * (offsets - centre)[None, None, :]
    cos_angle = jnp.cos(angle)
    sin_angle = jnp.sin(angle)
    phase = rotation[:, :, None] * (offsets + 1.0)[None, None, :]
    cos_phase = jnp.cos(phase)
    sin_phase = jnp.sin(phase)

    def advance(carry, pieces):
        carry_re, carry_im = carry
        part_re, part_im, shift_part, grouped_part = pieces
        level = jnp.dot(shift_part, triangle, precision=highest)
        log_from = level[:, None, :] - decay_rate[:, :, None] * (offsets + 1.0)[None, None, :]
        relative = log_from - log_from[:, :, centre : centre + 1]
        shrink = jnp.exp(-relative)
        lift_re = shrink * (part_re * cos_angle + part_im * sin_angle)
        lift_im = shrink * (part_im * cos_angle - part_re * sin_angle)
        prefix_re = jnp.dot(lift_re.reshape(groups * state_dim, BLOCK), triangle, precision=highest)
        prefix_im = jnp.dot(lift_im.reshape(groups * state_dim, BLOCK), triangle, precision=highest)
        prefix_re = prefix_re.reshape(groups, state_dim, BLOCK)
        prefix_im = prefix_im.reshape(groups, state_dim, BLOCK)
        grow = jnp.exp(relative)
        from_start = jnp.exp(log_from)
        keep_re = from_start * cos_phase
        keep_im = from_start * sin_phase
        state_re = grow * (prefix_re * cos_angle - prefix_im * sin_angle)
        state_im = grow * (prefix_im * cos_angle + prefix_re * sin_angle)
        state_re = state_re + keep_re * carry_re[:, :, None] - keep_im * carry_im[:, :, None]
        state_im = state_im + keep_re * carry_im[:, :, None] + keep_im * carry_re[:, :, None]
        result = jnp.einsum("ghp,gpt->ght", read_re, state_re, precision=highest)
        result = result - jnp.einsum("ghp,gpt->ght", read_im, state_im, precision=highest)
        result = result + skip_scale[:, :, None] * grouped_part.astype(jnp.float32)
        return ((state_re[:, :, -1], state_im[:, :, -1]), jax.nn.gelu(result).astype(jnp.bfloat16))

    drive_blocks = jnp.transpose(drive.reshape(groups, 2 * state_dim, blocks, BLOCK), (2, 0, 1, 3))
    shift_blocks = jnp.transpose(shift_cols.reshape(groups, blocks, BLOCK), (1, 0, 2))
    grouped_blocks = jnp.transpose(
        drive_cols.reshape(groups, GROUP_CH, blocks, BLOCK), (2, 0, 1, 3)
    )
    _, state_blocks = lax.scan(
        advance,
        (carried[2], carried[3]),
        (
            drive_blocks[:, :, :state_dim],
            drive_blocks[:, :, state_dim:],
            shift_blocks,
            grouped_blocks,
        ),
    )
    state_out = jnp.transpose(state_blocks, (0, 3, 1, 2)).reshape(length, channels)
    column_state, column_attend = (
        lax.all_gather(out_state, "sp", axis=1, tiled=True),
        lax.all_gather(out_attend, "sp", axis=1, tiled=True),
    )
    result = jnp.dot(state_out, column_state, preferred_element_type=jnp.float32)
    return lax.psum_scatter(
        (result + jnp.dot(attend_out, column_attend, preferred_element_type=jnp.float32)).astype(
            jnp.bfloat16
        ),
        "tp",
        scatter_dimension=0,
        tiled=True,
    )


MESH = pl.DeviceIdType.MESH
ANY = pl.BlockSpec(memory_space=pl.ANY)


def remote(src, dst, send, recv, **where):
    return pltpu.make_async_remote_copy(
        src_ref=src, dst_ref=dst, send_sem=send, recv_sem=recv, device_id=where, device_id_type=MESH
    )


def greet(peers):
    barrier = pltpu.get_barrier_semaphore()
    for peer in peers:
        pl.semaphore_signal(barrier, inc=1, device_id=peer, device_id_type=MESH)
    pl.semaphore_wait(barrier, len(peers))


def spread_kernel(n, n_fs, n_tp, repeat_dev, x, ssm, query, kv, shift, ows, owa,
                  xg, w_ssm, w_query, w_kv, shift_g, ows_g, owa_g,
                  held_x, held_w, held_s, held_o, held_p,
                  x_send, x_recv, q_send, q_recv, xp_send, xp_recv, w_send, w_recv, f_send, f_recv,
                  s_send, s_recv, o_send, o_recv, in_sem, out_sem):
    k = lax.axis_index("sp")
    f = lax.axis_index("fs")
    t = lax.axis_index("tp")
    tokens, half = x.shape
    rows = ssm.shape[0]
    part = rows // n_fs
    cs, cq = w_ssm.shape[1], w_query.shape[1]
    groups = shift_g.shape[0]
    other = 1 - t
    peers = [{"sp": lax.rem(k + s, n)} for s in range(1, n)]
    peers += [{"fs": lax.rem(f + d, n_fs)} for d in range(1, n_fs)]
    peers += [{"tp": other}]
    greet(peers)
    order = sorted(range(1, n), key=lambda s: -min(s, n - s))

    def piece(which, place, span):
        if which == 0:
            return ssm.at[span, pl.ds(pl.multiple_of(place * cs, 128), cs)]
        if which == 1:
            return query.at[span, pl.ds(pl.multiple_of(place * cq, 128), cq)]
        return kv.at[lax.div(place, repeat_dev), span]

    dests = (w_ssm, w_query, w_kv)

    def x_at(j, side):
        return xg.at[pl.ds(pl.multiple_of(j * tokens, 128), tokens),
                     pl.ds(pl.multiple_of(side * half, 128), half)]

    copies = []
    for s in order:
        peer = lax.rem(k + s, n)
        for which in range(3):
            mine = pl.ds(pl.multiple_of(f * part, 16), part)
            into = pl.ds(pl.multiple_of(k * rows + f * part, 16), part)
            copies.append(remote(piece(which, peer, mine), dests[which].at[into],
                                 w_send.at[which, s - 1], w_recv.at[which, s - 1], sp=peer))
            copies[-1].start()
    partner = [remote(x, x_at(k, t), xp_send.at[0], xp_recv.at[0], tp=other)]
    partner[0].start()
    for s in order:
        peer = lax.rem(k + s, n)
        c = remote(shift.at[pl.ds(pl.multiple_of(peer * groups, 8), groups)],
                   shift_g.at[:, pl.ds(pl.multiple_of(k * tokens, 128), tokens)],
                   s_send.at[s - 1], s_recv.at[s - 1], sp=peer)
        c.start()
        copies.append(c)

    def hop(step, way):
        block = lax.rem(k - way * step + n, n)
        dst = x_at(block, t)
        src = x if step == 0 else dst
        to = lax.rem(k + way + n, n)
        i = 0 if way > 0 else 1
        active = jnp.logical_and(k + way >= 0, k + way < n)
        active = jnp.logical_and(active, jnp.logical_and(k - way * step >= 0, k - way * step < n))
        return active, remote(src, dst, x_send.at[i, step], x_recv.at[i, step], sp=to)

    def arrival(step, way):
        origin = k - way * (step + 1)
        block = x_at(lax.rem(origin + n, n), t)
        i = 0 if way > 0 else 1
        active = jnp.logical_and(origin >= 0, origin < n)
        c = remote(block, block, x_send.at[i, step], x_recv.at[i, step], sp=lax.rem(k - way + n, n))
        p = remote(block, block, q_send.at[i, step], q_recv.at[i, step], tp=other)
        return active, c, p

    def start_hops(step):
        for way in (1, -1):
            active, c = hop(step, way)

            @pl.when(active)
            def _():
                c.start()

    start_hops(0)
    o_rows = pl.ds(pl.multiple_of(t * ows.shape[0], 16), ows.shape[0])
    for i, (src, dst) in enumerate(((ows, ows_g), (owa, owa_g))):
        c = remote(src, dst.at[o_rows], o_send.at[i], o_recv.at[i], tp=other)
        c.start()
        copies.append(c)
    everything = pl.ds(0, rows)
    here = pl.ds(pl.multiple_of(k * rows, 16), rows)
    local = [(x, held_x, x_at(k, t))]
    for which in range(3):
        local.append((piece(which, k, everything), held_w.at[which], dests[which].at[here]))
    local.append((shift.at[pl.ds(pl.multiple_of(k * groups, 8), groups)], held_s,
                  shift_g.at[:, pl.ds(pl.multiple_of(k * tokens, 128), tokens)]))
    local.append((ows, held_o, ows_g.at[o_rows]))
    local.append((owa, held_p, owa_g.at[o_rows]))
    ins = [pltpu.make_async_copy(a, b, in_sem.at[i]) for i, (a, b, _) in enumerate(local)]
    outs = [pltpu.make_async_copy(b, c, out_sem.at[i]) for i, (_, b, c) in enumerate(local)]
    for c in ins:
        c.start()
    for a, b in zip(ins, outs):
        a.wait()
        b.start()
    forwards = []
    for i, s in enumerate(sorted(range(1, n), key=lambda s: min(s, n - s))):
        source = lax.rem(k + n - s, n)
        into = pl.ds(pl.multiple_of(source * rows + f * part, 16), part)
        for which in range(3):
            got = dests[which].at[into]
            remote(got, got, w_send.at[which, s - 1], w_recv.at[which, s - 1], sp=source).wait_recv()
            for d in range(1, n_fs):
                c = remote(got, got, f_send.at[which, s - 1, d - 1], f_recv.at[which, s - 1, d - 1],
                           fs=lax.rem(f + d, n_fs))
                c.start()
                forwards.append(c)
    for step in range(n - 1):
        for way in (1, -1):
            active, c, p = arrival(step, way)

            @pl.when(active)
            def _():
                c.wait_recv()
                p.start()

        if step + 1 < n - 1:
            start_hops(step + 1)
    for step in range(n - 1):
        for way in (1, -1):
            active, c = hop(step, way)

            @pl.when(active)
            def _():
                c.wait_send()

            active, _c, p = arrival(step, way)

            @pl.when(active)
            def _():
                p.wait()

    for c in copies:
        c.wait_send()
    for c in copies[3 * (n - 1):]:
        c.wait_recv()
    for c in partner + forwards:
        c.wait()
    for c in outs:
        c.wait()


def spread(n, n_fs, n_tp, repeat_dev, x, ssm, query, kv, shift, ows, owa):
    tokens, half = x.shape
    rows = ssm.shape[0]
    cs, cq, ck = ssm.shape[1] // n, query.shape[1] // n, kv.shape[2]
    groups = shift.shape[0] // n
    bf = jnp.bfloat16
    dma = pltpu.SemaphoreType.DMA
    return pl.pallas_call(
        functools.partial(spread_kernel, n, n_fs, n_tp, repeat_dev),
        out_shape=[
            jax.ShapeDtypeStruct((n * tokens, n_tp * half), bf),
            jax.ShapeDtypeStruct((n * rows, cs), bf),
            jax.ShapeDtypeStruct((n * rows, cq), bf),
            jax.ShapeDtypeStruct((n * rows, ck), bf),
            jax.ShapeDtypeStruct((groups, n * tokens), jnp.float32),
            jax.ShapeDtypeStruct((n_tp * ows.shape[0], ows.shape[1]), bf),
            jax.ShapeDtypeStruct((n_tp * owa.shape[0], owa.shape[1]), bf),
        ],
        in_specs=[ANY] * 7,
        out_specs=[ANY] * 7,
        scratch_shapes=[
            pltpu.VMEM(x.shape, bf),
            pltpu.VMEM((3, rows, cs), bf),
            pltpu.VMEM((groups, tokens), jnp.float32),
            pltpu.VMEM(ows.shape, bf),
            pltpu.VMEM(owa.shape, bf),
            dma((2, n - 1)), dma((2, n - 1)), dma((2, n - 1)), dma((2, n - 1)), dma((1,)), dma((1,)),
            dma((3, n - 1)), dma((3, n - 1)),
            dma((3, n - 1, n_fs - 1)), dma((3, n - 1, n_fs - 1)),
            dma((n - 1,)), dma((n - 1,)), dma((2,)), dma((2,)), dma((7,)), dma((7,)),
        ],
        compiler_params=pltpu.CompilerParams(collective_id=0, has_side_effects=True),
    )(x, ssm, query, kv, shift, ows, owa)


def finish_kernel(n, hs, ha, ows, owa, out, got, passing, mixed,
                  h_send, h_recv, p_send, p_recv, own_send, own_recv, o_send, o_recv, in_sem, out_sem):
    k = lax.axis_index("sp")
    t = lax.axis_index("tp")
    other = 1 - t
    sources = (hs, ha)
    chunks = [(i, r) for r in (1, 0) for i in range(2)]
    greet([{"sp": lax.rem(k + s, n)} for s in range(1, n)] + [{"tp": other}])

    def landing(j, i, r):
        return passing.at[i, j] if r else got.at[i, t * n + j]

    def hop(step, way, chunk):
        i, r = chunks[chunk]
        origin = k - way * step
        dst = landing(lax.rem(origin + n, n), i, r)
        src = dst
        if step == 0:
            src = sources[i].at[other if r else t]
        active = jnp.logical_and(k + way >= 0, k + way < n)
        active = jnp.logical_and(active, jnp.logical_and(origin >= 0, origin < n))
        w = 0 if way > 0 else 1
        return active, remote(src, dst, h_send.at[w, step, chunk], h_recv.at[w, step, chunk],
                              sp=lax.rem(k + way + n, n))

    def arrival(step, way, chunk):
        i, r = chunks[chunk]
        origin = k - way * (step + 1)
        active = jnp.logical_and(origin >= 0, origin < n)
        j = lax.rem(origin + n, n)
        w = 0 if way > 0 else 1
        block = landing(j, i, r)
        c = remote(block, block, h_send.at[w, step, chunk], h_recv.at[w, step, chunk],
                   sp=lax.rem(k - way + n, n))
        p = None
        if r:
            p = remote(block, got.at[i, t * n + j], p_send.at[w, step, i], p_recv.at[w, step, i],
                       tp=other)
        return active, c, p

    for chunk in range(4):
        for way in (1, -1):
            active, c = hop(0, way, chunk)

            @pl.when(active)
            def _():
                c.start()

    own = []
    for i in range(2):
        c = remote(sources[i].at[other], got.at[i, t * n + k], own_send.at[i], own_recv.at[i], tp=other)
        c.start()
        own.append(c)
        c = pltpu.make_async_copy(sources[i].at[t], got.at[i, t * n + k], in_sem.at[i])
        c.start()
        own.append(c)
    for step in range(n - 1):
        for chunk in range(4):
            for way in (1, -1):
                active, c, p = arrival(step, way, chunk)

                @pl.when(active)
                def _():
                    c.wait_recv()
                    if p is not None:
                        p.start()

                if step + 1 < n - 1:
                    further, onward = hop(step + 1, way, chunk)

                    @pl.when(further)
                    def _():
                        onward.start()

    for step in range(n - 1):
        for chunk in range(4):
            for way in (1, -1):
                active, c = hop(step, way, chunk)

                @pl.when(active)
                def _():
                    c.wait_send()

                arrived, _c, p = arrival(step, way, chunk)
                if p is not None:

                    @pl.when(arrived)
                    def _():
                        p.wait()

    for c in own:
        c.wait()
    total = None
    for i, weights in enumerate((ows, owa)):
        rows = jnp.concatenate([got[i, j] for j in range(2 * n)], axis=1)
        term = jnp.dot(rows, weights[...], preferred_element_type=jnp.float32)
        total = term if total is None else total + term
    count, width = mixed.shape[1], mixed.shape[2]
    for j in range(n):
        mixed[j] = total[j * count : (j + 1) * count].astype(mixed.dtype)
    columns = pl.ds(pl.multiple_of(k * width, 128), width)
    copies = []
    for s in sorted(range(1, n), key=lambda s: -min(s, n - s)):
        peer = lax.rem(k + s, n)
        c = remote(mixed.at[peer], out.at[:, columns], o_send.at[s], o_recv.at[s], sp=peer)
        c.start()
        copies.append(c)
    c = pltpu.make_async_copy(mixed.at[k], out.at[:, columns], out_sem.at[0])
    c.start()
    c.wait()
    for c in copies:
        c.wait()


def finish(n, hs, ha, ows, owa):
    _, rows, width = hs.shape
    cols = ows.shape[1]
    dma = pltpu.SemaphoreType.DMA
    vmem = pl.BlockSpec(memory_space=pltpu.VMEM)
    bf = jnp.bfloat16
    return pl.pallas_call(
        functools.partial(finish_kernel, n),
        out_shape=jax.ShapeDtypeStruct((rows // n, n * cols), bf),
        in_specs=[vmem] * 4,
        out_specs=ANY,
        scratch_shapes=[
            pltpu.VMEM((2, 2 * n, rows, width), bf),
            pltpu.VMEM((2, n, rows, width), bf),
            pltpu.VMEM((n, rows // n, cols), bf),
            dma((2, n - 1, 4)), dma((2, n - 1, 4)), dma((2, n - 1, 2)), dma((2, n - 1, 2)),
            dma((2,)), dma((2,)), dma((n,)), dma((n,)), dma((2,)), dma((1,)),
        ],
        compiler_params=pltpu.CompilerParams(collective_id=1, has_side_effects=True),
    )(hs, ha, ows, owa)


def halves(x):
    high = x.astype(jnp.bfloat16)
    return high, (x - high.astype(jnp.float32)).astype(jnp.bfloat16)


def split_dot(x, exact):
    high, low = halves(x)
    return jnp.dot(high, exact, preferred_element_type=jnp.float32) + jnp.dot(
        low, exact, preferred_element_type=jnp.float32
    )


def column(row):
    size = row.shape[1]
    same = lax.broadcasted_iota(jnp.int32, (size, size), 0) == lax.broadcasted_iota(
        jnp.int32, (size, size), 1
    )
    return jnp.sum(jnp.where(same, row, 0.0), axis=1, keepdims=True)


def mixer_kernel(k, x, gain, w_ssm, w_query, w_kv, shift, rate, rotation, in_parts, out_parts,
                 skip, sinks, hs, ha, u_scr, q_scr, kv_scr, y_scr):
    f32, bf = jnp.float32, jnp.bfloat16
    length = x.shape[0]
    blocks = length // BLOCK
    groups = shift.shape[0]
    state = rate.shape[1]
    heads = w_query.shape[1] // HEAD_DIM
    side = BLOCK // 2
    kv_scr[0:WINDOW, :] = jnp.zeros((WINDOW, kv_scr.shape[1]), bf)

    for b in range(blocks):
        span = slice(b * BLOCK, (b + 1) * BLOCK)
        wide = x[span, :].astype(f32)
        scale = lax.rsqrt(jnp.mean(wide * wide, axis=1, keepdims=True) + epsilon)
        normed = (wide * scale * gain[...]).astype(bf)
        u = jnp.dot(normed, w_ssm[...], preferred_element_type=f32)
        u_scr[:, span] = jnp.transpose(u.astype(bf).astype(f32))
        q_scr[span, :] = jnp.dot(normed, w_query[...], preferred_element_type=f32).astype(bf)
        kv_scr[(b + 1) * BLOCK : (b + 2) * BLOCK, :] = jnp.dot(
            normed, w_kv[...], preferred_element_type=f32
        ).astype(bf)

    shape = (BLOCK, BLOCK)
    upto = lax.broadcasted_iota(jnp.int32, shape, 0) <= lax.broadcasted_iota(jnp.int32, shape, 1)
    tri = upto.astype(f32).astype(bf)
    centre = BLOCK // 2
    levels, lifts, grows, starts = [], [], [], []
    for b in range(blocks):
        part = shift[:, b * BLOCK : (b + 1) * BLOCK]
        high, low = halves(part)
        low2 = (part - high.astype(f32) - low.astype(f32)).astype(bf)
        level = (
            jnp.dot(high, tri, preferred_element_type=f32)
            + jnp.dot(low, tri, preferred_element_type=f32)
            + jnp.dot(low2, tri, preferred_element_type=f32)
        )
        middle = level[:, centre : centre + 1]
        lifts.append(jnp.exp(middle - level))
        grows.append(jnp.exp(level - middle))
        starts.append(jnp.exp(middle))
    away = lax.broadcasted_iota(jnp.int32, (state, BLOCK), 1).astype(f32) - float(centre)
    first = k * groups
    for g in range(groups):
        rates = column(rate[pl.ds(first + g, 1), :])
        turns = column(rotation[pl.ds(first + g, 1), :])
        angle = turns * away
        cos, sin = jnp.cos(angle), jnp.sin(angle)
        fade = jnp.exp(-rates * away)
        rise = jnp.exp(rates * away)
        up_re, up_im = rise * cos, -(rise * sin)
        down_re, down_im = fade * cos, fade * sin
        line, turn = rate[pl.ds(first + g, 1), :], rotation[pl.ds(first + g, 1), :]
        damped = jnp.exp(-line)
        lift_re = damped * jnp.cos(turn) - 1.0
        lift_im = damped * jnp.sin(turn)
        modulus = line * line + turn * turn
        factor_re = (turn * lift_im - line * lift_re) / modulus
        factor_im = -(turn * lift_re + line * lift_im) / modulus
        part_re = in_parts[0, g].astype(f32)
        part_im = in_parts[1, g].astype(f32)
        in_matrix = jnp.transpose(
            jnp.concatenate(
                [factor_re * part_re - factor_im * part_im, factor_re * part_im + factor_im * part_re],
                axis=1,
            )
        ).astype(bf)
        read = jnp.concatenate(
            [out_parts[0, g].astype(f32), -out_parts[1, g].astype(f32)], axis=1
        ).astype(bf)
        reach = jnp.exp(-rates * (centre + 1.0))
        reach_re = reach * jnp.cos(turns * (centre + 1.0))
        reach_im = reach * jnp.sin(turns * (centre + 1.0))
        u = u_scr[g * GROUP_CH : (g + 1) * GROUP_CH, :]
        drive = jnp.dot(in_matrix, u.astype(bf), preferred_element_type=f32)
        lifted = []
        for b in range(blocks):
            span = slice(b * BLOCK, (b + 1) * BLOCK)
            row = lifts[b][g : g + 1, :]
            d_re, d_im = drive[:state, span] * row, drive[state:, span] * row
            lifted += [d_re * up_re - d_im * up_im, d_re * up_im + d_im * up_re]
        prefix = split_dot(jnp.concatenate(lifted, axis=0), tri)
        carry_re = jnp.zeros((state, 1), f32)
        carry_im = carry_re
        chosen = lax.broadcasted_iota(jnp.int32, skip.shape, 1) == first + g
        skips = jnp.sum(jnp.where(chosen, skip[...], 0.0), axis=1, keepdims=True)
        for b in range(blocks):
            span = slice(b * BLOCK, (b + 1) * BLOCK)
            begin = starts[b][g : g + 1, :]
            base_re = begin * (carry_re * reach_re - carry_im * reach_im)
            base_im = begin * (carry_re * reach_im + carry_im * reach_re)
            p_re = prefix[2 * b * state : (2 * b + 1) * state] + base_re
            p_im = prefix[(2 * b + 1) * state : (2 * b + 2) * state] + base_im
            row = grows[b][g : g + 1, :]
            s_re = row * (down_re * p_re - down_im * p_im)
            s_im = row * (down_re * p_im + down_im * p_re)
            carry_re, carry_im = s_re[:, BLOCK - 1 :], s_im[:, BLOCK - 1 :]
            high, low = halves(jnp.concatenate([s_re, s_im], axis=0))
            y = jnp.dot(read, high, preferred_element_type=f32) + jnp.dot(
                read, low, preferred_element_type=f32
            )
            y_scr[g * GROUP_CH : (g + 1) * GROUP_CH, span] = y + skips * u[:, span]

    for b in range(blocks):
        y = y_scr[:, b * BLOCK : (b + 1) * BLOCK]
        y = jnp.transpose(jax.nn.gelu(y)).astype(bf)
        hs[0, b * side : (b + 1) * side, :] = y[:side]
        hs[1, b * side : (b + 1) * side, :] = y[side:]

    wide = (WINDOW, 2 * WINDOW)
    gap = lax.broadcasted_iota(jnp.int32, wide, 0) + WINDOW - lax.broadcasted_iota(jnp.int32, wide, 1)
    inside = (gap >= 0) & (gap < WINDOW)
    inside_first = inside & (lax.broadcasted_iota(jnp.int32, wide, 1) >= WINDOW)
    for b in range(blocks):
        keys = kv_scr[b * WINDOW : (b + 2) * WINDOW, :HEAD_DIM]
        values = kv_scr[b * WINDOW : (b + 2) * WINDOW, HEAD_DIM:]
        valid = inside if b else inside_first
        outs = []
        for h in range(heads):
            query = q_scr[b * WINDOW : (b + 1) * WINDOW, h * HEAD_DIM : (h + 1) * HEAD_DIM]
            scores = lax.dot_general(query, keys, (((1,), (1,)), ((), ())), preferred_element_type=f32)
            scores = jnp.where(valid, scores * HEAD_DIM ** (-0.5), floor_score)
            sink = sinks[k * heads + h]
            peak = jnp.maximum(jnp.max(scores, axis=1, keepdims=True), sink)
            raised = jnp.where(valid, jnp.exp(scores - peak), 0.0)
            total = jnp.sum(raised, axis=1, keepdims=True) + jnp.exp(sink - peak)
            weights = (raised / total).astype(bf)
            outs.append(jnp.dot(weights, values, preferred_element_type=f32))
        out = jnp.concatenate(outs, axis=1).astype(bf)
        ha[0, b * side : (b + 1) * side, :] = out[:side]
        ha[1, b * side : (b + 1) * side, :] = out[side:]


def mixer_entry(*refs):
    mixer_kernel(lax.axis_index("sp"), *refs)


def mixer(x, gain, w_ssm, w_query, w_kv, shift, rate, rotation, in_parts, out_parts, skip, sinks,
          entry=mixer_entry, interpret=False):
    length = x.shape[0]
    vmem = pl.BlockSpec(memory_space=pltpu.VMEM)
    return pl.pallas_call(
        entry,
        out_shape=[
            jax.ShapeDtypeStruct((2, length // 2, w_ssm.shape[1]), jnp.bfloat16),
            jax.ShapeDtypeStruct((2, length // 2, w_query.shape[1]), jnp.bfloat16),
        ],
        in_specs=[vmem] * 11 + [pl.BlockSpec(memory_space=pltpu.SMEM)],
        out_specs=[vmem] * 2,
        scratch_shapes=[
            pltpu.VMEM((w_ssm.shape[1], length), jnp.float32),
            pltpu.VMEM((length, w_query.shape[1]), jnp.bfloat16),
            pltpu.VMEM((length + WINDOW, w_kv.shape[1]), jnp.bfloat16),
            pltpu.VMEM((w_ssm.shape[1], length), jnp.float32),
        ],
        interpret=interpret,
    )(x, gain, w_ssm, w_query, w_kv, shift, rate, rotation, in_parts, out_parts, skip, sinks)


def fast_body(
    inputs, norm_gain, in_ssm, in_query, in_key, in_value, decay_rate, rotation, input_parts,
    output_parts, skip_scale, decay_shift, sink_logit, out_state, out_attend,
):
    n, n_fs, n_tp = lax.axis_size("sp"), lax.axis_size("fs"), lax.axis_size("tp")
    key_heads = in_key.shape[1] // HEAD_DIM
    kv = jnp.stack(
        [
            jnp.concatenate([array[:, h * HEAD_DIM : (h + 1) * HEAD_DIM] for array in (in_key, in_value)], axis=1)
            for h in range(key_heads)
        ]
    )
    gathered, w_ssm, w_query, w_kv, shift_cols, ows, owa = spread(
        n, n_fs, n_tp, n // key_heads, inputs, in_ssm, in_query, kv,
        jnp.transpose(decay_shift), out_state, out_attend,
    )

    def own(array):
        size = array.shape[1] // n
        return lax.dynamic_slice_in_dim(array, lax.axis_index("sp") * size, size, 1)

    by_side_state, by_side_attend = mixer(
        gathered, norm_gain[None], w_ssm, w_query, w_kv, shift_cols, decay_rate, rotation,
        own(jnp.swapaxes(input_parts, 2, 3)), own(output_parts), skip_scale.T, sink_logit,
    )
    return finish(n, by_side_state, by_side_attend, ows, owa)


def body(*args):
    n, n_fs, n_tp = lax.axis_size("sp"), lax.axis_size("fs"), lax.axis_size("tp")
    inputs, in_ssm, in_query, in_key, decay_rate = args[0], args[2], args[3], args[4], args[6]
    key_heads = in_key.shape[1] // HEAD_DIM
    query_heads = in_query.shape[1] // HEAD_DIM
    fits = (
        n_tp == 2
        and 1 < n <= 8
        and n_fs > 1
        and n % key_heads == 0
        and query_heads % n == 0
        and in_ssm.shape[1] == in_query.shape[1]
        and in_ssm.shape[1] % (128 * n) == 0
        and 2 * HEAD_DIM == in_ssm.shape[1] // n
        and decay_rate.shape[0] % (8 * n) == 0
        and decay_rate.shape[0] * GROUP_CH == in_ssm.shape[1]
        and inputs.shape[0] == BLOCK == WINDOW
        and inputs.shape[1] % 128 == 0
        and in_ssm.shape[0] % (16 * n_fs) == 0
        and args[13].shape[1] % 128 == 0
    )
    return (fast_body if fits else general_body)(*args)


def solution(mesh):
    return jax.shard_map(
        body,
        mesh=mesh,
        in_specs=(
            P(("fs", "sp"), "tp"),
            P(),
            P("sp", "tp"),
            P("sp", "tp"),
            P("sp", "tp"),
            P("sp", "tp"),
            P("tp", None),
            P("tp", None),
            P(None, "tp", None, None),
            P(None, "tp", None, None),
            P("tp", None),
            P(("fs", "sp"), "tp"),
            P("tp"),
            P("tp", "sp"),
            P("tp", "sp"),
        ),
        out_specs=P(("fs", "sp", "tp"), None),
        check_vma=False,
    )
```

```python
import functools
import jax
import jax.numpy as jnp
from jax import lax
from jax.experimental import pallas as pl
from jax.experimental.pallas import tpu as pltpu
from jax.sharding import PartitionSpec as P

GROUP_CH = 16
HEAD_DIM = 64
WINDOW = 128
BLOCK = 128


epsilon = 1e-06
floor_score = -1e30


def prefix(x, axis, join, neutral):
    place = lax.axis_index(axis)
    gathered = jax.tree.map(
        lambda a, kind: lax.all_gather(a.astype(kind), axis),
        x,
        (jnp.bfloat16, jnp.bfloat16, jnp.bfloat16, jnp.bfloat16),
    )
    state = jax.tree.map(lambda a, e: jnp.zeros_like(a) + jnp.asarray(e, a.dtype), x, neutral)

    def one(hop, state):
        return join(
            state,
            jax.tree.map(
                lambda a, own: lax.dynamic_index_in_dim(a, hop, 0, False).astype(own.dtype),
                gathered,
                x,
            ),
        )

    return lax.fori_loop(0, place, one, state)


def from_behind(value, axis, steps):
    count = lax.axis_size(axis)
    initial, last = (max(0, -steps), min(count, count - steps))
    return lax.ppermute(value, axis, [(source, source + steps) for source in range(initial, last)])


def combine(earlier, later):
    first_re, first_im, state_re, state_im = earlier
    second_re, second_im, input_re, input_im = later
    return (
        second_re * first_re - second_im * first_im,
        second_re * first_im + second_im * first_re,
        second_re * state_re - second_im * state_im + input_re,
        second_re * state_im + second_im * state_re + input_im,
    )


def input_matrix(decay_rate, rotation, input_parts):
    damped = jnp.exp(-decay_rate)
    lift_re = damped * jnp.cos(rotation) - 1.0
    lift_im = damped * jnp.sin(rotation)
    modulus = decay_rate * decay_rate + rotation * rotation
    factor_re = (rotation * lift_im - decay_rate * lift_re) / modulus
    factor_im = -(rotation * lift_re + decay_rate * lift_im) / modulus
    part_re = input_parts[0].astype(jnp.float32)
    part_im = input_parts[1].astype(jnp.float32)
    joined_re = factor_re[:, :, None] * part_re - factor_im[:, :, None] * part_im
    joined_im = factor_re[:, :, None] * part_im + factor_im[:, :, None] * part_re
    return jnp.concatenate([joined_re, joined_im], axis=1).astype(jnp.bfloat16)


def window_attention(queries, keys_win, values_win, starts, sink_logit):
    window = queries.shape[1]
    scores = jnp.einsum("nqgrd,nkgd->ngrqk", queries, keys_win, preferred_element_type=jnp.float32)
    scores = scores * queries.shape[-1] ** (-0.5)
    places = (
        jnp.arange(window, dtype=jnp.int32)[:, None]
        + window
        - jnp.arange(2 * window, dtype=jnp.int32)[None, :]
    )
    inside = (places >= 0) & (places < window)
    reach = starts[:, None] - window + jnp.arange(2 * window, dtype=jnp.int32)[None, :] >= 0
    valid = (inside[None] & reach[:, None, :])[:, None, None]
    sinks = sink_logit.reshape(scores.shape[1], scores.shape[2])[None, :, :, None, None]
    scores = jnp.where(valid, scores, floor_score)
    row_peak = jnp.maximum(jnp.max(scores, axis=-1, keepdims=True), sinks)
    raised = jnp.where(valid, jnp.exp(scores - row_peak), 0.0)
    denominator = jnp.sum(raised, axis=-1, keepdims=True) + jnp.exp(sinks - row_peak)
    weights = (raised / denominator).astype(jnp.bfloat16)
    result = jnp.einsum(
        "ngrqk,nkgd->nqgrd", weights, values_win, preferred_element_type=jnp.float32
    )
    return result.astype(jnp.bfloat16)


def general_body(
    inputs,
    norm_gain,
    in_ssm,
    in_query,
    in_key,
    in_value,
    decay_rate,
    rotation,
    input_parts,
    output_parts,
    skip_scale,
    decay_shift,
    sink_logit,
    out_state,
    out_attend,
):
    gathered = lax.all_gather(inputs, "tp", axis=1, tiled=True)
    length = gathered.shape[0]
    widened = gathered.astype(jnp.float32)
    scale = lax.rsqrt(jnp.mean(widened * widened, axis=1, keepdims=True) + epsilon)
    normed = (widened * scale * norm_gain).astype(jnp.bfloat16)

    def add_rows(pieces):
        return tuple(
            (jnp.dot(normed, piece, preferred_element_type=jnp.float32) for piece in pieces)
        )

    projected = add_rows(
        (
            lax.all_gather(in_ssm, "sp", axis=0, tiled=True),
            lax.all_gather(in_query, "sp", axis=0, tiled=True),
            lax.all_gather(in_key, "sp", axis=0, tiled=True),
            lax.all_gather(in_value, "sp", axis=0, tiled=True),
        )
    )
    drive_in, queries, keys_local, values = [piece.astype(jnp.bfloat16) for piece in projected]
    groups = decay_rate.shape[0]
    state_dim = decay_rate.shape[1]
    channels = groups * GROUP_CH
    highest = lax.Precision.HIGHEST
    drive_cols = jnp.transpose(drive_in).reshape(groups, GROUP_CH, length)
    in_matrix = input_matrix(decay_rate, rotation, input_parts)
    drive = jnp.einsum("gqh,ght->gqt", in_matrix, drive_cols, preferred_element_type=jnp.float32)
    shift_cols = jnp.transpose(decay_shift)
    running = jnp.cumsum(shift_cols, axis=1)
    total_shift = running[:, -1]
    remain = length - 1.0 - jnp.arange(length, dtype=jnp.float32)
    to_end = (total_shift[:, None] - running)[:, None, :] - decay_rate[:, :, None] * remain[
        None, None, :
    ]
    fade = jnp.exp(to_end)
    turn = rotation[:, :, None] * remain[None, None, :]
    weight_re = fade * jnp.cos(turn)
    weight_im = fade * jnp.sin(turn)
    drive_re = drive[:, :state_dim]
    drive_im = drive[:, state_dim:]
    final_re = jnp.sum(weight_re * drive_re - weight_im * drive_im, axis=2)
    final_im = jnp.sum(weight_re * drive_im + weight_im * drive_re, axis=2)
    overall = jnp.exp(total_shift[:, None] - decay_rate * length)
    nothing = jnp.zeros_like(final_re)
    carried = prefix(
        (
            overall * jnp.cos(rotation * length),
            overall * jnp.sin(rotation * length),
            final_re,
            final_im,
        ),
        "sp",
        combine,
        (jnp.ones_like(final_re), nothing, nothing, nothing),
    )
    key_heads = keys_local.shape[1] // HEAD_DIM
    query_heads = queries.shape[1] // HEAD_DIM
    windows_dev = length // WINDOW
    previous = from_behind((keys_local, values), "sp", 1)

    def windows(flat, before):
        split = jnp.concatenate([before, flat], axis=0).reshape(
            windows_dev + 1, WINDOW, key_heads, HEAD_DIM
        )
        return jnp.concatenate([split[:-1], split[1:]], axis=1)

    offset = lax.axis_index("sp") * length
    starts = offset + jnp.arange(windows_dev, dtype=jnp.int32) * WINDOW
    queries_blk = queries.reshape(
        windows_dev, WINDOW, key_heads, query_heads // key_heads, HEAD_DIM
    )
    attended = window_attention(
        queries_blk,
        windows(keys_local, previous[0]),
        windows(values, previous[1]),
        starts,
        sink_logit,
    )
    attend_out = attended.reshape(length, query_heads * HEAD_DIM)
    blocks = length // BLOCK
    triangle = (
        jnp.arange(BLOCK, dtype=jnp.int32)[:, None] <= jnp.arange(BLOCK, dtype=jnp.int32)[None, :]
    ).astype(jnp.float32)
    offsets = jnp.arange(BLOCK, dtype=jnp.float32)
    centre = BLOCK // 2
    read_re = output_parts[0].astype(jnp.float32)
    read_im = output_parts[1].astype(jnp.float32)
    angle = rotation[:, :, None] * (offsets - centre)[None, None, :]
    cos_angle = jnp.cos(angle)
    sin_angle = jnp.sin(angle)
    phase = rotation[:, :, None] * (offsets + 1.0)[None, None, :]
    cos_phase = jnp.cos(phase)
    sin_phase = jnp.sin(phase)

    def advance(carry, pieces):
        carry_re, carry_im = carry
        part_re, part_im, shift_part, grouped_part = pieces
        level = jnp.dot(shift_part, triangle, precision=highest)
        log_from = level[:, None, :] - decay_rate[:, :, None] * (offsets + 1.0)[None, None, :]
        relative = log_from - log_from[:, :, centre : centre + 1]
        shrink = jnp.exp(-relative)
        lift_re = shrink * (part_re * cos_angle + part_im * sin_angle)
        lift_im = shrink * (part_im * cos_angle - part_re * sin_angle)
        prefix_re = jnp.dot(lift_re.reshape(groups * state_dim, BLOCK), triangle, precision=highest)
        prefix_im = jnp.dot(lift_im.reshape(groups * state_dim, BLOCK), triangle, precision=highest)
        prefix_re = prefix_re.reshape(groups, state_dim, BLOCK)
        prefix_im = prefix_im.reshape(groups, state_dim, BLOCK)
        grow = jnp.exp(relative)
        from_start = jnp.exp(log_from)
        keep_re = from_start * cos_phase
        keep_im = from_start * sin_phase
        state_re = grow * (prefix_re * cos_angle - prefix_im * sin_angle)
        state_im = grow * (prefix_im * cos_angle + prefix_re * sin_angle)
        state_re = state_re + keep_re * carry_re[:, :, None] - keep_im * carry_im[:, :, None]
        state_im = state_im + keep_re * carry_im[:, :, None] + keep_im * carry_re[:, :, None]
        result = jnp.einsum("ghp,gpt->ght", read_re, state_re, precision=highest)
        result = result - jnp.einsum("ghp,gpt->ght", read_im, state_im, precision=highest)
        result = result + skip_scale[:, :, None] * grouped_part.astype(jnp.float32)
        return ((state_re[:, :, -1], state_im[:, :, -1]), jax.nn.gelu(result).astype(jnp.bfloat16))

    drive_blocks = jnp.transpose(drive.reshape(groups, 2 * state_dim, blocks, BLOCK), (2, 0, 1, 3))
    shift_blocks = jnp.transpose(shift_cols.reshape(groups, blocks, BLOCK), (1, 0, 2))
    grouped_blocks = jnp.transpose(
        drive_cols.reshape(groups, GROUP_CH, blocks, BLOCK), (2, 0, 1, 3)
    )
    _, state_blocks = lax.scan(
        advance,
        (carried[2], carried[3]),
        (
            drive_blocks[:, :, :state_dim],
            drive_blocks[:, :, state_dim:],
            shift_blocks,
            grouped_blocks,
        ),
    )
    state_out = jnp.transpose(state_blocks, (0, 3, 1, 2)).reshape(length, channels)
    column_state, column_attend = (
        lax.all_gather(out_state, "sp", axis=1, tiled=True),
        lax.all_gather(out_attend, "sp", axis=1, tiled=True),
    )
    result = jnp.dot(state_out, column_state, preferred_element_type=jnp.float32)
    return lax.psum_scatter(
        (result + jnp.dot(attend_out, column_attend, preferred_element_type=jnp.float32)).astype(
            jnp.bfloat16
        ),
        "tp",
        scatter_dimension=0,
        tiled=True,
    )


MESH = pl.DeviceIdType.MESH
ANY = pl.BlockSpec(memory_space=pl.ANY)


def remote(src, dst, send, recv, **where):
    return pltpu.make_async_remote_copy(
        src_ref=src, dst_ref=dst, send_sem=send, recv_sem=recv, device_id=where, device_id_type=MESH
    )


def greet(peers):
    barrier = pltpu.get_barrier_semaphore()
    for peer in peers:
        pl.semaphore_signal(barrier, inc=1, device_id=peer, device_id_type=MESH)
    pl.semaphore_wait(barrier, len(peers))


def spread_kernel(n, n_fs, n_tp, repeat_dev, x, ssm, query, kv, shift, ows, owa,
                  xg, w_ssm, w_query, w_kv, shift_g, ows_g, owa_g,
                  held_x, held_w, held_s, held_o, held_p,
                  x_send, x_recv, q_send, q_recv, xp_send, xp_recv, w_send, w_recv, f_send, f_recv,
                  s_send, s_recv, o_send, o_recv, in_sem, out_sem):
    k = lax.axis_index("sp")
    f = lax.axis_index("fs")
    t = lax.axis_index("tp")
    tokens, half = x.shape
    rows = ssm.shape[0]
    part = rows // n_fs
    cs, cq = w_ssm.shape[1], w_query.shape[1]
    groups = shift_g.shape[0]
    other = 1 - t
    peers = [{"sp": lax.rem(k + s, n)} for s in range(1, n)]
    peers += [{"fs": lax.rem(f + d, n_fs)} for d in range(1, n_fs)]
    peers += [{"tp": other}]
    greet(peers)
    order = sorted(range(1, n), key=lambda s: -min(s, n - s))

    def piece(which, place, span):
        if which == 0:
            return ssm.at[span, pl.ds(pl.multiple_of(place * cs, 128), cs)]
        if which == 1:
            return query.at[span, pl.ds(pl.multiple_of(place * cq, 128), cq)]
        return kv.at[lax.div(place, repeat_dev), span]

    dests = (w_ssm, w_query, w_kv)

    def x_at(j, side):
        return xg.at[pl.ds(pl.multiple_of(j * tokens, 128), tokens),
                     pl.ds(pl.multiple_of(side * half, 128), half)]

    copies = []
    for s in order:
        peer = lax.rem(k + s, n)
        for which in range(3):
            mine = pl.ds(pl.multiple_of(f * part, 16), part)
            into = pl.ds(pl.multiple_of(k * rows + f * part, 16), part)
            copies.append(remote(piece(which, peer, mine), dests[which].at[into],
                                 w_send.at[which, s - 1], w_recv.at[which, s - 1], sp=peer))
            copies[-1].start()
    partner = [remote(x, x_at(k, t), xp_send.at[0], xp_recv.at[0], tp=other)]
    partner[0].start()
    for s in order:
        peer = lax.rem(k + s, n)
        c = remote(shift.at[pl.ds(pl.multiple_of(peer * groups, 8), groups)],
                   shift_g.at[:, pl.ds(pl.multiple_of(k * tokens, 128), tokens)],
                   s_send.at[s - 1], s_recv.at[s - 1], sp=peer)
        c.start()
        copies.append(c)

    def hop(step, way):
        block = lax.rem(k - way * step + n, n)
        dst = x_at(block, t)
        src = x if step == 0 else dst
        to = lax.rem(k + way + n, n)
        i = 0 if way > 0 else 1
        active = jnp.logical_and(k + way >= 0, k + way < n)
        active = jnp.logical_and(active, jnp.logical_and(k - way * step >= 0, k - way * step < n))
        return active, remote(src, dst, x_send.at[i, step], x_recv.at[i, step], sp=to)

    def arrival(step, way):
        origin = k - way * (step + 1)
        block = x_at(lax.rem(origin + n, n), t)
        i = 0 if way > 0 else 1
        active = jnp.logical_and(origin >= 0, origin < n)
        c = remote(block, block, x_send.at[i, step], x_recv.at[i, step], sp=lax.rem(k - way + n, n))
        p = remote(block, block, q_send.at[i, step], q_recv.at[i, step], tp=other)
        return active, c, p

    def start_hops(step):
        for way in (1, -1):
            active, c = hop(step, way)

            @pl.when(active)
            def _():
                c.start()

    start_hops(0)
    o_rows = pl.ds(pl.multiple_of(t * ows.shape[0], 16), ows.shape[0])
    for i, (src, dst) in enumerate(((ows, ows_g), (owa, owa_g))):
        c = remote(src, dst.at[o_rows], o_send.at[i], o_recv.at[i], tp=other)
        c.start()
        copies.append(c)
    everything = pl.ds(0, rows)
    here = pl.ds(pl.multiple_of(k * rows, 16), rows)
    local = [(x, held_x, x_at(k, t))]
    for which in range(3):
        local.append((piece(which, k, everything), held_w.at[which], dests[which].at[here]))
    local.append((shift.at[pl.ds(pl.multiple_of(k * groups, 8), groups)], held_s,
                  shift_g.at[:, pl.ds(pl.multiple_of(k * tokens, 128), tokens)]))
    local.append((ows, held_o, ows_g.at[o_rows]))
    local.append((owa, held_p, owa_g.at[o_rows]))
    ins = [pltpu.make_async_copy(a, b, in_sem.at[i]) for i, (a, b, _) in enumerate(local)]
    outs = [pltpu.make_async_copy(b, c, out_sem.at[i]) for i, (_, b, c) in enumerate(local)]
    for c in ins:
        c.start()
    for a, b in zip(ins, outs):
        a.wait()
        b.start()
    forwards = []
    for i, s in enumerate(sorted(range(1, n), key=lambda s: min(s, n - s))):
        source = lax.rem(k + n - s, n)
        into = pl.ds(pl.multiple_of(source * rows + f * part, 16), part)
        for which in range(3):
            got = dests[which].at[into]
            remote(got, got, w_send.at[which, s - 1], w_recv.at[which, s - 1], sp=source).wait_recv()
            for d in range(1, n_fs):
                c = remote(got, got, f_send.at[which, s - 1, d - 1], f_recv.at[which, s - 1, d - 1],
                           fs=lax.rem(f + d, n_fs))
                c.start()
                forwards.append(c)
    for step in range(n - 1):
        for way in (1, -1):
            active, c, p = arrival(step, way)

            @pl.when(active)
            def _():
                c.wait_recv()
                p.start()

        if step + 1 < n - 1:
            start_hops(step + 1)
    for step in range(n - 1):
        for way in (1, -1):
            active, c = hop(step, way)

            @pl.when(active)
            def _():
                c.wait_send()

            active, _c, p = arrival(step, way)

            @pl.when(active)
            def _():
                p.wait()

    for c in copies:
        c.wait_send()
    for c in copies[3 * (n - 1):]:
        c.wait_recv()
    for c in partner + forwards:
        c.wait()
    for c in outs:
        c.wait()


def spread(n, n_fs, n_tp, repeat_dev, x, ssm, query, kv, shift, ows, owa):
    tokens, half = x.shape
    rows = ssm.shape[0]
    cs, cq, ck = ssm.shape[1] // n, query.shape[1] // n, kv.shape[2]
    groups = shift.shape[0] // n
    bf = jnp.bfloat16
    dma = pltpu.SemaphoreType.DMA
    return pl.pallas_call(
        functools.partial(spread_kernel, n, n_fs, n_tp, repeat_dev),
        out_shape=[
            jax.ShapeDtypeStruct((n * tokens, n_tp * half), bf),
            jax.ShapeDtypeStruct((n * rows, cs), bf),
            jax.ShapeDtypeStruct((n * rows, cq), bf),
            jax.ShapeDtypeStruct((n * rows, ck), bf),
            jax.ShapeDtypeStruct((groups, n * tokens), jnp.float32),
            jax.ShapeDtypeStruct((n_tp * ows.shape[0], ows.shape[1]), bf),
            jax.ShapeDtypeStruct((n_tp * owa.shape[0], owa.shape[1]), bf),
        ],
        in_specs=[ANY] * 7,
        out_specs=[ANY] * 7,
        scratch_shapes=[
            pltpu.VMEM(x.shape, bf),
            pltpu.VMEM((3, rows, cs), bf),
            pltpu.VMEM((groups, tokens), jnp.float32),
            pltpu.VMEM(ows.shape, bf),
            pltpu.VMEM(owa.shape, bf),
            dma((2, n - 1)), dma((2, n - 1)), dma((2, n - 1)), dma((2, n - 1)), dma((1,)), dma((1,)),
            dma((3, n - 1)), dma((3, n - 1)),
            dma((3, n - 1, n_fs - 1)), dma((3, n - 1, n_fs - 1)),
            dma((n - 1,)), dma((n - 1,)), dma((2,)), dma((2,)), dma((7,)), dma((7,)),
        ],
        compiler_params=pltpu.CompilerParams(collective_id=0, has_side_effects=True),
    )(x, ssm, query, kv, shift, ows, owa)


def finish_kernel(n, hs, ha, ows, owa, out, got, passing, mixed,
                  h_send, h_recv, p_send, p_recv, own_send, own_recv, o_send, o_recv, in_sem, out_sem):
    k = lax.axis_index("sp")
    t = lax.axis_index("tp")
    other = 1 - t
    sources = (hs, ha)
    chunks = [(i, r) for r in (1, 0) for i in range(2)]
    greet([{"sp": lax.rem(k + s, n)} for s in range(1, n)] + [{"tp": other}])

    def landing(j, i, r):
        return passing.at[i, j] if r else got.at[i, t * n + j]

    def hop(step, way, chunk):
        i, r = chunks[chunk]
        origin = k - way * step
        dst = landing(lax.rem(origin + n, n), i, r)
        src = dst
        if step == 0:
            src = sources[i].at[other if r else t]
        active = jnp.logical_and(k + way >= 0, k + way < n)
        active = jnp.logical_and(active, jnp.logical_and(origin >= 0, origin < n))
        w = 0 if way > 0 else 1
        return active, remote(src, dst, h_send.at[w, step, chunk], h_recv.at[w, step, chunk],
                              sp=lax.rem(k + way + n, n))

    def arrival(step, way, chunk):
        i, r = chunks[chunk]
        origin = k - way * (step + 1)
        active = jnp.logical_and(origin >= 0, origin < n)
        j = lax.rem(origin + n, n)
        w = 0 if way > 0 else 1
        block = landing(j, i, r)
        c = remote(block, block, h_send.at[w, step, chunk], h_recv.at[w, step, chunk],
                   sp=lax.rem(k - way + n, n))
        p = None
        if r:
            p = remote(block, got.at[i, t * n + j], p_send.at[w, step, i], p_recv.at[w, step, i],
                       tp=other)
        return active, c, p

    for chunk in range(4):
        for way in (1, -1):
            active, c = hop(0, way, chunk)

            @pl.when(active)
            def _():
                c.start()

    own = []
    for i in range(2):
        c = remote(sources[i].at[other], got.at[i, t * n + k], own_send.at[i], own_recv.at[i], tp=other)
        c.start()
        own.append(c)
        c = pltpu.make_async_copy(sources[i].at[t], got.at[i, t * n + k], in_sem.at[i])
        c.start()
        own.append(c)
    for step in range(n - 1):
        for chunk in range(4):
            for way in (1, -1):
                active, c, p = arrival(step, way, chunk)

                @pl.when(active)
                def _():
                    c.wait_recv()
                    if p is not None:
                        p.start()

                if step + 1 < n - 1:
                    further, onward = hop(step + 1, way, chunk)

                    @pl.when(further)
                    def _():
                        onward.start()

    for step in range(n - 1):
        for chunk in range(4):
            for way in (1, -1):
                active, c = hop(step, way, chunk)

                @pl.when(active)
                def _():
                    c.wait_send()

                arrived, _c, p = arrival(step, way, chunk)
                if p is not None:

                    @pl.when(arrived)
                    def _():
                        p.wait()

    for c in own:
        c.wait()
    total = None
    for i, weights in enumerate((ows, owa)):
        rows = jnp.concatenate([got[i, j] for j in range(2 * n)], axis=1)
        term = jnp.dot(rows, weights[...], preferred_element_type=jnp.float32)
        total = term if total is None else total + term
    count, width = mixed.shape[1], mixed.shape[2]
    for j in range(n):
        mixed[j] = total[j * count : (j + 1) * count].astype(mixed.dtype)
    columns = pl.ds(pl.multiple_of(k * width, 128), width)
    copies = []
    for s in sorted(range(1, n), key=lambda s: -min(s, n - s)):
        peer = lax.rem(k + s, n)
        c = remote(mixed.at[peer], out.at[:, columns], o_send.at[s], o_recv.at[s], sp=peer)
        c.start()
        copies.append(c)
    c = pltpu.make_async_copy(mixed.at[k], out.at[:, columns], out_sem.at[0])
    c.start()
    c.wait()
    for c in copies:
        c.wait()


def finish(n, hs, ha, ows, owa):
    _, rows, width = hs.shape
    cols = ows.shape[1]
    dma = pltpu.SemaphoreType.DMA
    vmem = pl.BlockSpec(memory_space=pltpu.VMEM)
    bf = jnp.bfloat16
    return pl.pallas_call(
        functools.partial(finish_kernel, n),
        out_shape=jax.ShapeDtypeStruct((rows // n, n * cols), bf),
        in_specs=[vmem] * 4,
        out_specs=ANY,
        scratch_shapes=[
            pltpu.VMEM((2, 2 * n, rows, width), bf),
            pltpu.VMEM((2, n, rows, width), bf),
            pltpu.VMEM((n, rows // n, cols), bf),
            dma((2, n - 1, 4)), dma((2, n - 1, 4)), dma((2, n - 1, 2)), dma((2, n - 1, 2)),
            dma((2,)), dma((2,)), dma((n,)), dma((n,)), dma((2,)), dma((1,)),
        ],
        compiler_params=pltpu.CompilerParams(collective_id=1, has_side_effects=True),
    )(hs, ha, ows, owa)


def halves(x):
    high = x.astype(jnp.bfloat16)
    return high, (x - high.astype(jnp.float32)).astype(jnp.bfloat16)


def split_dot(x, exact):
    high, low = halves(x)
    return jnp.dot(high, exact, preferred_element_type=jnp.float32) + jnp.dot(
        low, exact, preferred_element_type=jnp.float32
    )


def column(row):
    size = row.shape[1]
    same = lax.broadcasted_iota(jnp.int32, (size, size), 0) == lax.broadcasted_iota(
        jnp.int32, (size, size), 1
    )
    return jnp.sum(jnp.where(same, row, 0.0), axis=1, keepdims=True)


def mixer_kernel(k, x, gain, w_ssm, w_query, w_kv, shift, rate, rotation, in_parts, out_parts,
                 skip, sinks, hs, ha, u_scr, q_scr, kv_scr, y_scr):
    f32, bf = jnp.float32, jnp.bfloat16
    length = x.shape[0]
    blocks = length // BLOCK
    groups = shift.shape[0]
    state = rate.shape[1]
    heads = w_query.shape[1] // HEAD_DIM
    side = BLOCK // 2
    kv_scr[0:WINDOW, :] = jnp.zeros((WINDOW, kv_scr.shape[1]), bf)

    for b in range(blocks):
        span = slice(b * BLOCK, (b + 1) * BLOCK)
        wide = x[span, :].astype(f32)
        scale = lax.rsqrt(jnp.mean(wide * wide, axis=1, keepdims=True) + epsilon)
        normed = (wide * scale * gain[...]).astype(bf)
        u = jnp.dot(normed, w_ssm[...], preferred_element_type=f32)
        u_scr[:, span] = jnp.transpose(u.astype(bf).astype(f32))
        q_scr[span, :] = jnp.dot(normed, w_query[...], preferred_element_type=f32).astype(bf)
        kv_scr[(b + 1) * BLOCK : (b + 2) * BLOCK, :] = jnp.dot(
            normed, w_kv[...], preferred_element_type=f32
        ).astype(bf)

    shape = (BLOCK, BLOCK)
    upto = lax.broadcasted_iota(jnp.int32, shape, 0) <= lax.broadcasted_iota(jnp.int32, shape, 1)
    tri = upto.astype(f32).astype(bf)
    centre = BLOCK // 2
    levels, lifts, grows, starts = [], [], [], []
    for b in range(blocks):
        part = shift[:, b * BLOCK : (b + 1) * BLOCK]
        high, low = halves(part)
        low2 = (part - high.astype(f32) - low.astype(f32)).astype(bf)
        level = (
            jnp.dot(high, tri, preferred_element_type=f32)
            + jnp.dot(low, tri, preferred_element_type=f32)
            + jnp.dot(low2, tri, preferred_element_type=f32)
        )
        middle = level[:, centre : centre + 1]
        lifts.append(jnp.exp(middle - level))
        grows.append(jnp.exp(level - middle))
        starts.append(jnp.exp(middle))
    away = lax.broadcasted_iota(jnp.int32, (state, BLOCK), 1).astype(f32) - float(centre)
    first = k * groups
    for g in range(groups):
        rates = column(rate[pl.ds(first + g, 1), :])
        turns = column(rotation[pl.ds(first + g, 1), :])
        angle = turns * away
        cos, sin = jnp.cos(angle), jnp.sin(angle)
        fade = jnp.exp(-rates * away)
        rise = jnp.exp(rates * away)
        up_re, up_im = rise * cos, -(rise * sin)
        down_re, down_im = fade * cos, fade * sin
        line, turn = rate[pl.ds(first + g, 1), :], rotation[pl.ds(first + g, 1), :]
        damped = jnp.exp(-line)
        lift_re = damped * jnp.cos(turn) - 1.0
        lift_im = damped * jnp.sin(turn)
        modulus = line * line + turn * turn
        factor_re = (turn * lift_im - line * lift_re) / modulus
        factor_im = -(turn * lift_re + line * lift_im) / modulus
        part_re = in_parts[0, g].astype(f32)
        part_im = in_parts[1, g].astype(f32)
        in_matrix = jnp.transpose(
            jnp.concatenate(
                [factor_re * part_re - factor_im * part_im, factor_re * part_im + factor_im * part_re],
                axis=1,
            )
        ).astype(bf)
        read = jnp.concatenate(
            [out_parts[0, first + g].astype(f32), -out_parts[1, first + g].astype(f32)], axis=1
        ).astype(bf)
        reach = jnp.exp(-rates * (centre + 1.0))
        reach_re = reach * jnp.cos(turns * (centre + 1.0))
        reach_im = reach * jnp.sin(turns * (centre + 1.0))
        u = u_scr[g * GROUP_CH : (g + 1) * GROUP_CH, :]
        drive = jnp.dot(in_matrix, u.astype(bf), preferred_element_type=f32)
        lifted = []
        for b in range(blocks):
            span = slice(b * BLOCK, (b + 1) * BLOCK)
            row = lifts[b][g : g + 1, :]
            d_re, d_im = drive[:state, span] * row, drive[state:, span] * row
            lifted += [d_re * up_re - d_im * up_im, d_re * up_im + d_im * up_re]
        prefix = split_dot(jnp.concatenate(lifted, axis=0), tri)
        carry_re = jnp.zeros((state, 1), f32)
        carry_im = carry_re
        chosen = lax.broadcasted_iota(jnp.int32, skip.shape, 1) == first + g
        skips = jnp.sum(jnp.where(chosen, skip[...], 0.0), axis=1, keepdims=True)
        for b in range(blocks):
            span = slice(b * BLOCK, (b + 1) * BLOCK)
            begin = starts[b][g : g + 1, :]
            base_re = begin * (carry_re * reach_re - carry_im * reach_im)
            base_im = begin * (carry_re * reach_im + carry_im * reach_re)
            p_re = prefix[2 * b * state : (2 * b + 1) * state] + base_re
            p_im = prefix[(2 * b + 1) * state : (2 * b + 2) * state] + base_im
            row = grows[b][g : g + 1, :]
            s_re = row * (down_re * p_re - down_im * p_im)
            s_im = row * (down_re * p_im + down_im * p_re)
            carry_re, carry_im = s_re[:, BLOCK - 1 :], s_im[:, BLOCK - 1 :]
            high, low = halves(jnp.concatenate([s_re, s_im], axis=0))
            y = jnp.dot(read, high, preferred_element_type=f32) + jnp.dot(
                read, low, preferred_element_type=f32
            )
            y_scr[g * GROUP_CH : (g + 1) * GROUP_CH, span] = y + skips * u[:, span]

    for b in range(blocks):
        y = y_scr[:, b * BLOCK : (b + 1) * BLOCK]
        y = jnp.transpose(jax.nn.gelu(y)).astype(bf)
        hs[0, b * side : (b + 1) * side, :] = y[:side]
        hs[1, b * side : (b + 1) * side, :] = y[side:]

    wide = (WINDOW, 2 * WINDOW)
    gap = lax.broadcasted_iota(jnp.int32, wide, 0) + WINDOW - lax.broadcasted_iota(jnp.int32, wide, 1)
    inside = (gap >= 0) & (gap < WINDOW)
    inside_first = inside & (lax.broadcasted_iota(jnp.int32, wide, 1) >= WINDOW)
    for b in range(blocks):
        keys = kv_scr[b * WINDOW : (b + 2) * WINDOW, :HEAD_DIM]
        values = kv_scr[b * WINDOW : (b + 2) * WINDOW, HEAD_DIM:]
        valid = inside if b else inside_first
        outs = []
        for h in range(heads):
            query = q_scr[b * WINDOW : (b + 1) * WINDOW, h * HEAD_DIM : (h + 1) * HEAD_DIM]
            scores = lax.dot_general(query, keys, (((1,), (1,)), ((), ())), preferred_element_type=f32)
            scores = jnp.where(valid, scores * HEAD_DIM ** (-0.5), floor_score)
            sink = sinks[k * heads + h]
            peak = jnp.maximum(jnp.max(scores, axis=1, keepdims=True), sink)
            raised = jnp.where(valid, jnp.exp(scores - peak), 0.0)
            total = jnp.sum(raised, axis=1, keepdims=True) + jnp.exp(sink - peak)
            weights = (raised / total).astype(bf)
            outs.append(jnp.dot(weights, values, preferred_element_type=f32))
        out = jnp.concatenate(outs, axis=1).astype(bf)
        ha[0, b * side : (b + 1) * side, :] = out[:side]
        ha[1, b * side : (b + 1) * side, :] = out[side:]


def mixer_entry(*refs):
    mixer_kernel(lax.axis_index("sp"), *refs)


def mixer(x, gain, w_ssm, w_query, w_kv, shift, rate, rotation, in_parts, out_parts, skip, sinks,
          entry=mixer_entry, interpret=False):
    length = x.shape[0]
    vmem = pl.BlockSpec(memory_space=pltpu.VMEM)
    return pl.pallas_call(
        entry,
        out_shape=[
            jax.ShapeDtypeStruct((2, length // 2, w_ssm.shape[1]), jnp.bfloat16),
            jax.ShapeDtypeStruct((2, length // 2, w_query.shape[1]), jnp.bfloat16),
        ],
        in_specs=[vmem] * 11 + [pl.BlockSpec(memory_space=pltpu.SMEM)],
        out_specs=[vmem] * 2,
        scratch_shapes=[
            pltpu.VMEM((w_ssm.shape[1], length), jnp.float32),
            pltpu.VMEM((length, w_query.shape[1]), jnp.bfloat16),
            pltpu.VMEM((length + WINDOW, w_kv.shape[1]), jnp.bfloat16),
            pltpu.VMEM((w_ssm.shape[1], length), jnp.float32),
        ],
        interpret=interpret,
    )(x, gain, w_ssm, w_query, w_kv, shift, rate, rotation, in_parts, out_parts, skip, sinks)


def fast_body(
    inputs, norm_gain, in_ssm, in_query, in_key, in_value, decay_rate, rotation, input_parts,
    output_parts, skip_scale, decay_shift, sink_logit, out_state, out_attend,
):
    n, n_fs, n_tp = lax.axis_size("sp"), lax.axis_size("fs"), lax.axis_size("tp")
    key_heads = in_key.shape[1] // HEAD_DIM
    kv = jnp.stack(
        [
            jnp.concatenate([array[:, h * HEAD_DIM : (h + 1) * HEAD_DIM] for array in (in_key, in_value)], axis=1)
            for h in range(key_heads)
        ]
    )
    gathered, w_ssm, w_query, w_kv, shift_cols, ows, owa = spread(
        n, n_fs, n_tp, n // key_heads, inputs, in_ssm, in_query, kv,
        jnp.transpose(decay_shift), out_state, out_attend,
    )

    def own(array):
        size = array.shape[1] // n
        return lax.dynamic_slice_in_dim(array, lax.axis_index("sp") * size, size, 1)

    by_side_state, by_side_attend = mixer(
        gathered, norm_gain[None], w_ssm, w_query, w_kv, shift_cols, decay_rate, rotation,
        own(jnp.swapaxes(input_parts, 2, 3)), output_parts, skip_scale.T, sink_logit,
    )
    return finish(n, by_side_state, by_side_attend, ows, owa)


def body(*args):
    n, n_fs, n_tp = lax.axis_size("sp"), lax.axis_size("fs"), lax.axis_size("tp")
    inputs, in_ssm, in_query, in_key, decay_rate = args[0], args[2], args[3], args[4], args[6]
    key_heads = in_key.shape[1] // HEAD_DIM
    query_heads = in_query.shape[1] // HEAD_DIM
    fits = (
        n_tp == 2
        and 1 < n <= 8
        and n_fs > 1
        and n % key_heads == 0
        and query_heads % n == 0
        and in_ssm.shape[1] == in_query.shape[1]
        and in_ssm.shape[1] % (128 * n) == 0
        and 2 * HEAD_DIM == in_ssm.shape[1] // n
        and decay_rate.shape[0] % (8 * n) == 0
        and decay_rate.shape[0] * GROUP_CH == in_ssm.shape[1]
        and inputs.shape[0] == BLOCK == WINDOW
        and inputs.shape[1] % 128 == 0
        and in_ssm.shape[0] % (16 * n_fs) == 0
        and args[13].shape[1] % 128 == 0
    )
    return (fast_body if fits else general_body)(*args)


def solution(mesh):
    return jax.shard_map(
        body,
        mesh=mesh,
        in_specs=(
            P(("fs", "sp"), "tp"),
            P(),
            P("sp", "tp"),
            P("sp", "tp"),
            P("sp", "tp"),
            P("sp", "tp"),
            P("tp", None),
            P("tp", None),
            P(None, "tp", None, None),
            P(None, "tp", None, None),
            P("tp", None),
            P(("fs", "sp"), "tp"),
            P("tp"),
            P("tp", "sp"),
            P("tp", "sp"),
        ),
        out_specs=P(("fs", "sp", "tp"), None),
        check_vma=False,
    )
```
